128 devices in a mesh: rep: 2 (over z_hi), fs: 32 (over z_lo, y, x), tp: 2 (over core).
Axes of the slice: x: 4, y: 4, z: 4 (z_hi: 2, z_lo: 2; z = z_hi * 2 + z_lo), core: 2. Of those that a mesh axis runs over, the one named last changes fastest.
Arguments:
- hidden_in: bfloat16 [49152, 2048], P(('rep', 'fs', 'tp')), may hold values from -6 to 6
- norm_gain: float32 [2048], replicated, may hold values from 0.1 to 1.9
- up_weight: float32 [2048, 8192], P('fs', 'tp'), may hold values from -0.125 to 0.125
- up_scale: float32 [8192], P('tp'), may hold values from 0.5 to 2
- down_weight: float32 [8192, 2048], P('tp', 'fs'), may hold values from -0.0625 to 0.0625
- down_scale: float32 [2048], replicated, may hold values from 0.5 to 2
Outputs:
- layer_out: bfloat16 [49152, 2048], P(('rep', 'fs', 'tp'))
The draws below stay inside these ranges and needn't reach their ends.
All inputs are finite; a program needn't handle non-finite values.
Results may differ from the reference program's by a relative error of at most 0.0085.
Values may be sent and summed in bfloat16 or wider, within the bound.
No kernel may reach another device: no remote copies, remote signals or barrier semaphores. Data moves between devices by JAX's collectives and lax.ppermute only.
A program may use at most 128 MiB of HBM per device.

```python
import math
import jax
import jax.numpy as jnp
from jax import lax

D = 2048
FF = 8192
TOKENS = 49152
N_TP = 2


def shard_levels(rng, shape, split, smallest, high):
    def one(dim, parts):
        draws = jax.random.uniform(jax.random.fold_in(jax.random.fold_in(rng, 6), dim), (parts,), jnp.float32, smallest / len(split), high / len(split))
        return jnp.repeat(jnp.exp(draws), shape[dim] // parts).reshape((-1,) + (1,) * (len(shape) - dim - 1))

    level = one(*split[0])
    for cut in split[1:]:
        level = level * one(*cut)
    return level


def normal_values(stream_key, shape, deviation, most, pieces=(), kind=jnp.bfloat16):
    level = shard_levels(stream_key, shape, pieces, -0.22, 0.18) if pieces else 1.0
    values = jax.random.normal(stream_key, shape, jnp.float32) * deviation * level
    return jnp.minimum(jnp.maximum(values, -most), most).astype(kind)


def setup_inputs(seed: int = 0) -> dict:
    seeds = jax.random.split(jax.random.key(seed), 7)
    return {
        "hidden_in": normal_values(seeds[0], (TOKENS, D), 1.0, 6.0, ((0, 128),)),
        "norm_gain": jnp.clip(1.0 + 0.18 * jax.random.normal(seeds[1], (D,), jnp.float32), 0.1, 1.9),
        "up_weight": normal_values(seeds[2], (D, FF), D ** -0.5, 0.125, ((0, 32), (1, 2)), jnp.float32),
        "up_scale": jnp.clip(jnp.exp(math.log(2.0) - 1.3862944 * jax.random.uniform(seeds[3], (FF,), jnp.float32) ** shard_levels(seeds[3], (FF,), ((0, 2),), -0.2, 0.2)), 0.5, 2.0),
        "down_weight": normal_values(seeds[4], (FF, D), FF ** -0.5, 0.0625, ((0, 2), (1, 32)), jnp.float32),
        "down_scale": jnp.clip(jnp.exp(jax.random.uniform(seeds[5], (D,), jnp.float32, math.log(0.5), math.log(2.0))), 0.5, 2.0),
    }


def reference(hidden_in, norm_gain, up_weight, up_scale, down_weight, down_scale):
    up_low = up_weight.astype(jnp.bfloat16)
    down_low = down_weight.astype(jnp.bfloat16)
    block = math.gcd(2048, TOKENS)
    width = FF // N_TP

    def one_block(start):
        rows = lax.dynamic_slice_in_dim(hidden_in, start, block, 0).astype(jnp.float32)
        normed = (rows * lax.rsqrt(lax.optimization_barrier(jnp.mean(rows * rows, axis=1, keepdims=True)) + 1e-06) * norm_gain).astype(jnp.bfloat16)
        pre = jnp.dot(normed, up_low, preferred_element_type=jnp.float32) * up_scale
        act = jnp.square(jnp.maximum(pre, 0.0)).astype(jnp.bfloat16)
        total = jnp.zeros((block, D), jnp.float32)
        for index in range(N_TP):
            part = jnp.dot(act[:, index * width:(index + 1) * width], down_low[index * width:(index + 1) * width], preferred_element_type=jnp.float32).astype(jnp.bfloat16)
            part = lax.optimization_barrier(part)
            total = total + part.astype(jnp.float32)
        return (total * down_scale).astype(jnp.bfloat16)
    starts = jnp.arange(0, TOKENS, block, dtype=jnp.int32)
    outs = lax.map(one_block, starts)
    return outs.reshape(TOKENS, D)
```

```python
import jax
import jax.numpy as jnp
from jax import lax
from jax.sharding import Mesh, PartitionSpec as P

Z = ("zh", "zl")
UP = [(0, 1), (1, 2), (2, 3), (3, 0)]
DOWN = [(1, 0), (2, 1), (3, 2), (0, 3)]
SWAP = [(0, 1), (1, 0)]


def body(hidden_in, norm_gain, up_weight, up_scale, down_weight, down_scale):
    zl = lax.axis_index("zl")
    tokens, width = hidden_in.shape
    units = up_weight.shape[1] // 2
    half = tokens // 2
    pair = jnp.stack([up_weight.astype(jnp.bfloat16), down_weight.astype(jnp.bfloat16).T])
    mine = lax.dynamic_slice_in_dim(pair, zl * units, units, 2)
    theirs = lax.dynamic_slice_in_dim(pair, (1 - zl) * units, units, 2)
    rows = pair.shape[1]
    low = lax.ppermute(theirs[:, : rows // 2], Z, UP)
    high = lax.ppermute(theirs[:, rows // 2 :], Z, DOWN)
    other = jnp.concatenate([low, high], axis=1)
    swap = zl == 1
    first = jnp.where(swap, other, mine)
    second = jnp.where(swap, mine, other)

    f32 = hidden_in.astype(jnp.float32)
    normed = (
        f32 * lax.rsqrt(jnp.mean(f32 * f32, axis=1, keepdims=True) + 1e-06) * norm_gain
    ).astype(jnp.bfloat16)
    from_below = lax.ppermute(normed[:half], Z, UP)
    from_above = lax.ppermute(normed[half:], Z, DOWN)
    held = jnp.concatenate([normed, from_below, from_above], axis=0)
    x = jnp.concatenate([held, lax.ppermute(held, "c", SWAP)], axis=0)

    def gathered(index):
        shard = jnp.stack([first[index], second[index]])
        return lax.all_gather(shard, ("y", "x"), axis=1, tiled=True).reshape(width, units)

    up_whole = gathered(0)
    pre = jnp.dot(x, up_whole, preferred_element_type=jnp.float32)
    scale = lax.dynamic_slice_in_dim(up_scale, zl * units, units, 0)
    act = jnp.square(jnp.maximum(pre * scale, 0.0)).astype(jnp.bfloat16)
    down_whole = gathered(1)
    part = lax.dot_general(act, down_whole, (((1,), (1,)), ((), ())), preferred_element_type=jnp.float32)
    part = part.astype(jnp.bfloat16)
    kept, sent = part[: 2 * tokens], part[2 * tokens :]
    summed = kept.astype(jnp.float32) + lax.ppermute(sent, "c", SWAP).astype(jnp.float32)
    own, low, high = summed[:tokens], summed[tokens : tokens + half], summed[tokens + half :]
    back_high = lax.ppermute(low.astype(jnp.bfloat16), Z, DOWN)
    back_low = lax.ppermute(high.astype(jnp.bfloat16), Z, UP)
    total = own + jnp.concatenate([back_high, back_low], axis=0).astype(jnp.float32)
    return (total * down_scale).astype(jnp.bfloat16)


def solution(mesh):
    fine = Mesh(mesh.devices.reshape(2, 2, 4, 4, 2), ("zh", "zl", "y", "x", "c"))
    fs = ("zl", "y", "x")
    rows = P(("zh", "zl", "y", "x", "c"), None)
    placed = (rows, P(), P(fs, "c"), P("c"), P("c", fs), P())
    return jax.shard_map(body, mesh=fine, in_specs=placed, out_specs=rows, check_vma=False)
```

```python
import functools

import jax
import jax.numpy as jnp
from jax import lax
from jax.experimental import pallas as pl
from jax.experimental.pallas import tpu as pltpu
from jax.sharding import Mesh, PartitionSpec as P

AXES = ("zh", "zl", "y", "x", "c")
NEAR = (0, -1, 1, 2)
BLOCK = 64
LINE = 4 * BLOCK
ROWS = 512
ANY = pl.BlockSpec(memory_space=pl.ANY)
SMEM = pl.BlockSpec(memory_space=pltpu.SMEM)
VMEM = pl.BlockSpec(memory_space=pltpu.VMEM)
BF16 = jnp.bfloat16


def index_of(z, y, x, c):
    return ((z % 4 * 4 + y % 4) * 4 + x % 4) * 2 + c


def pairs_of(target):
    pairs = []
    for z in range(4):
        for y in range(4):
            for x in range(4):
                for c in range(2):
                    to = target(z, y, x, c)
                    if to is not None:
                        pairs.append((index_of(z, y, x, c), index_of(*to)))
    return pairs


def first_ring(d):
    return pairs_of(lambda z, y, x, c: (z, y + d, x, c) if c else (z, y, x + d, c))


def second_ring(d):
    return pairs_of(lambda z, y, x, c: (z, y, x + d, c) if c else (z, y + d, x, c))


def z_ring(d):
    return pairs_of(lambda z, y, x, c: (z + d, y, x, c))


FIRST = (first_ring(1), first_ring(-1))
SECOND = (second_ring(1), second_ring(-1))
UPWARD, DOWNWARD = z_ring(1), z_ring(-1)
SWAP = pairs_of(lambda z, y, x, c: (z, y, x, 1 - c))


def to_lower(z, y, x, c):
    if c == 0:
        return z - 1, y, x, z % 2
    return (z, y, x, 0) if z % 2 == 0 else None


def to_upper(z, y, x, c):
    if c == 1:
        return z + 1, y, x, z % 2
    return (z, y, x, 1) if z % 2 == 1 else None


TO_LOWER, TO_UPPER = pairs_of(to_lower), pairs_of(to_upper)


def send(a, pairs):
    return lax.ppermute(a, AXES, pairs)


def around(own, ring):
    before, after = send(own, ring[0]), send(own, ring[1])
    n = own.shape[0] // 2
    return own, before, after, send(before[:n], ring[0]), send(after[n:], ring[1])


def near(value, shift):
    return lax.rem(value + (shift + 4), 4)


def parts_of(refs):
    own, before, after, low, high = refs
    out = [(ref, i, d, e) for d, ref in ((0, own), (-1, before), (1, after)) for i, e in enumerate(NEAR)]
    return out + [(low, 0, 2, 0), (low, 1, 2, -1), (high, 0, 2, 1), (high, 1, 2, 2)]


def up_kernel(first, pos, x0, x1, scale, a0, a1, a2, a3, a4, act, xv, wv, ov, xsem, wsem, osem):
    a, b, sa, sb, core = pos[0], pos[1], pos[2], pos[3], pos[4]
    rows, width = xv.shape
    n = wv.shape[1]
    chunk = 256
    held = rows // 2
    mine, other = pl.multiple_of(core * held, held), pl.multiple_of((1 - core) * held, held)
    for j in range(n // chunk):
        cols, src_cols = pl.ds(j * chunk, chunk), pl.ds(first + j * chunk, chunk)
        for ref, i, d, e in parts_of((a0, a1, a2, a3, a4)):
            for level in range(2):
                at = pl.multiple_of(level * (width // 2) + near(a, e) * sa + near(b, d) * sb, BLOCK)
                pltpu.make_async_copy(
                    ref.at[pl.ds((2 * i + level) * BLOCK, BLOCK), src_cols], wv.at[pl.ds(at, BLOCK), cols], wsem.at[j]
                ).start()
        if j == 0:
            pltpu.make_async_copy(x0, xv.at[pl.ds(mine, held)], xsem.at[0]).start()
            pltpu.make_async_copy(x1, xv.at[pl.ds(other, held)], xsem.at[1]).start()
    outs = []
    for j in range(n // chunk):
        cols = pl.ds(j * chunk, chunk)
        pltpu.make_async_copy(wv.at[:, cols], wv.at[:, cols], wsem.at[j]).wait()
        if j == 0:
            pltpu.make_async_copy(x0, xv.at[pl.ds(mine, held)], xsem.at[0]).wait()
            pltpu.make_async_copy(x1, xv.at[pl.ds(other, held)], xsem.at[1]).wait()

        def one(k, carry, cols=cols):
            r = pl.ds(pl.multiple_of(k * ROWS, ROWS), ROWS)
            pre = jnp.dot(xv[r, :], wv[:, cols], preferred_element_type=jnp.float32)
            pre = jnp.maximum(pre * scale[:, cols], 0.0)
            ov[r, cols] = (pre * pre).astype(BF16)
            return carry

        lax.fori_loop(0, rows // ROWS, one, 0)
        out = pltpu.make_async_copy(ov.at[:, cols], act.at[:, cols], osem.at[j])
        out.start()
        outs.append(out)
    for out in outs:
        out.wait()


def up_call(part, pos, x0, x1, scale, weights):
    rows, width = 2 * x0.shape[0], x0.shape[1]
    n = scale.shape[1]
    return pl.pallas_call(
        functools.partial(up_kernel, part * n),
        name=f"up{part}",
        out_shape=jax.ShapeDtypeStruct((rows, n), BF16),
        in_specs=[SMEM, ANY, ANY, VMEM] + [ANY] * 5,
        out_specs=ANY,
        scratch_shapes=[
            pltpu.VMEM((rows, width), BF16),
            pltpu.VMEM((width, n), BF16),
            pltpu.VMEM((rows, n), BF16),
            pltpu.SemaphoreType.DMA((2,)),
            pltpu.SemaphoreType.DMA((n // 256,)),
            pltpu.SemaphoreType.DMA((n // 256,)),
        ],
        compiler_params=pltpu.CompilerParams(vmem_limit_bytes=24 * 2**20),
        cost_estimate=pl.CostEstimate(flops=2 * rows * width * n, bytes_accessed=2 * (rows * width + width * n + rows * n), transcendentals=0),
    )(pos, x0, x1, scale, *weights)


def down_kernel(batch, pos, h0, h1, o0, o1, *refs):
    n_refs = (3, 2)[batch]
    refs, (own, low, high, av, vv, ov, asem, vsem, osem) = refs[:n_refs], refs[n_refs:]
    a = pos[0]
    rows = av.shape[0]
    quarter = av.shape[1] // 4
    if batch == 0:
        blocks = [(ref, i, g, e) for g, ref in enumerate(refs) for i, e in enumerate(NEAR)]
    else:
        blocks = [(refs[0], 0, 0, 0), (refs[0], 1, 0, -1), (refs[1], 0, 0, 1), (refs[1], 1, 0, 2)]
    for ref, i, g, e in blocks:
        at = pl.multiple_of(g * LINE + near(a, e) * BLOCK, BLOCK)
        pltpu.make_async_copy(ref.at[pl.ds(i * BLOCK, BLOCK)], vv.at[pl.ds(at, BLOCK)], vsem.at[g]).start()

    def a_copy(k, q, ref):
        r = pl.ds(k * ROWS, ROWS)
        return pltpu.make_async_copy(ref.at[r], av.at[r, pl.ds(q * quarter, quarter)], asem.at[4 * k + q])

    sources = list(enumerate((h0, h1, o0, o1)))
    for k in range(rows // ROWS):
        for q, ref in sources:
            a_copy(k, q, ref).start()
    for g in range(vv.shape[0] // LINE):
        cols = pl.ds(g * LINE, LINE)
        pltpu.make_async_copy(vv.at[cols], vv.at[cols], vsem.at[g]).wait()
        for k in range(rows // ROWS):
            if g == 0:
                for q, ref in sources:
                    a_copy(k, q, ref).wait()
            r = pl.ds(k * ROWS, ROWS)
            part = lax.dot_general(
                av[r, :], vv[cols, :], (((1,), (1,)), ((), ())), preferred_element_type=jnp.float32
            )
            ov[r, cols] = part.astype(BF16)
    held = rows // 2
    kept = held // 2
    half = kept // 2
    outs = []
    for c in range(2):
        for ref, start, size in ((own, 0, kept), (low, kept, half), (high, kept + half, half)):
            outs.append(
                pltpu.make_async_copy(
                    ov.at[pl.ds(c * held + start, size)], ref.at[pl.ds(c * size, size)], osem.at[len(outs)]
                )
            )
    for out in outs:
        out.start()
    for out in outs:
        out.wait()


COLUMNS = (3 * LINE, LINE)


def down_call(batch, pos, act, refs):
    rows, units = act[0].shape[0], 4 * act[0].shape[1]
    n = COLUMNS[batch]
    return pl.pallas_call(
        functools.partial(down_kernel, batch),
        name=f"down{batch}",
        out_shape=[jax.ShapeDtypeStruct((rows // k, n), BF16) for k in (2, 4, 4)],
        in_specs=[SMEM] + [ANY] * (4 + len(refs)),
        out_specs=[ANY] * 3,
        scratch_shapes=[
            pltpu.VMEM((rows, units), BF16),
            pltpu.VMEM((n, units), BF16),
            pltpu.VMEM((rows, n), BF16),
            pltpu.SemaphoreType.DMA((4 * rows // ROWS,)),
            pltpu.SemaphoreType.DMA((3,)),
            pltpu.SemaphoreType.DMA((6,)),
        ],
        compiler_params=pltpu.CompilerParams(vmem_limit_bytes=32 * 2**20),
        cost_estimate=pl.CostEstimate(flops=2 * rows * units * n, bytes_accessed=2 * (rows * units + units * n + rows * n), transcendentals=0),
    )(pos, *act, *refs)


def sum_kernel(pos, own, above, below, gain, mine, theirs):
    core = pos[4]
    kept = mine.shape[0]
    half = kept // 2
    for ref, who in ((mine, core), (theirs, 1 - core)):
        for i, other in enumerate((above, below)):
            r = pl.ds(pl.multiple_of(who * kept + i * half, half), half)
            total = own[r, :].astype(jnp.float32) + other[pl.ds(pl.multiple_of(who * half, half), half), :].astype(jnp.float32)
            ref[pl.ds(i * half, half), :] = (total * gain[...]).astype(BF16)


def sum_call(batch, pos, own, above, below, gain):
    shape = jax.ShapeDtypeStruct((own.shape[0] // 2, own.shape[1]), BF16)
    return pl.pallas_call(
        sum_kernel,
        name=f"sum{batch}",
        out_shape=[shape, shape],
        in_specs=[SMEM, VMEM, VMEM, VMEM, VMEM],
        out_specs=[VMEM, VMEM],
        compiler_params=pltpu.CompilerParams(vmem_limit_bytes=16 * 2**20),
    )(pos, own, above, below, gain)


def last_kernel(pos, m0, m1, g0, g1, out, qv, ov, dsem, qsem, osem):
    core, y, x = pos[4], pos[5], pos[6]
    half = ov.shape[1]

    def pieces(wide, narrow):
        refs = ((wide, 0), (wide, 1), (wide, 2), (narrow, 0))
        return [(ref.at[:, pl.ds(i * LINE, LINE)], d) for (ref, i), d in zip(refs, NEAR)]

    def start(straight, mixed):
        for ref, d in straight:
            at = pl.multiple_of(near(y, d) * LINE, LINE)
            pltpu.make_async_copy(ref, out.at[:, pl.ds(at, LINE)], dsem.at[0]).start()
        for ref, d in mixed:
            pltpu.make_async_copy(ref, qv.at[near(x, d)], qsem.at[0]).start()

    @pl.when(core == 0)
    def _():
        start(pieces(m0, m1), pieces(g0, g1))

    @pl.when(core == 1)
    def _():
        start(pieces(g0, g1), pieces(m0, m1))

    pltpu.make_async_copy(qv, qv, qsem.at[0]).wait()
    left = lax.broadcasted_iota(jnp.int32, (qv.shape[1], 128), 1) < BLOCK
    for pair in range(2):
        for v in range(2):
            cols = pl.ds(128 * v, 128)
            even = qv[2 * pair, :, cols].astype(jnp.float32)
            odd = qv[2 * pair + 1, :, cols].astype(jnp.float32)
            ov[:, pl.ds(2 * v * LINE + pair * 128, 128)] = jnp.where(left, even, pltpu.roll(odd, BLOCK, 1)).astype(BF16)
            ov[:, pl.ds((2 * v + 1) * LINE + pair * 128, 128)] = jnp.where(left, pltpu.roll(even, BLOCK, 1), odd).astype(BF16)
    copy = pltpu.make_async_copy(ov, out.at[:, pl.ds(half, half)], osem.at[0])
    copy.start()
    copy.wait()
    pltpu.make_async_copy(ov, out.at[:, pl.ds(0, half)], dsem.at[0]).wait()


def last_call(pos, *refs):
    rows = refs[0].shape[0]
    return pl.pallas_call(
        last_kernel,
        name="last",
        out_shape=jax.ShapeDtypeStruct((rows, 8 * LINE), BF16),
        in_specs=[SMEM] + [ANY] * 4,
        out_specs=ANY,
        scratch_shapes=[
            pltpu.VMEM((4, rows, LINE), BF16),
            pltpu.VMEM((rows, 4 * LINE), BF16),
            pltpu.SemaphoreType.DMA((1,)),
            pltpu.SemaphoreType.DMA((1,)),
            pltpu.SemaphoreType.DMA((1,)),
        ],
        compiler_params=pltpu.CompilerParams(vmem_limit_bytes=16 * 2**20),
    )(pos, *refs)


def body(hidden_in, norm_gain, up_weight, up_scale, down_weight, down_scale):
    zl, y, x, core = (lax.axis_index(name) for name in ("zl", "y", "x", "c"))
    a, b = jnp.where(core == 0, x, y), jnp.where(core == 0, y, x)
    sa, sb = jnp.where(core == 0, BLOCK, LINE), jnp.where(core == 0, LINE, BLOCK)
    pos = jnp.stack([a, b, sa, sb, core, y, x]).astype(jnp.int32)
    tokens, width = hidden_in.shape
    units = up_weight.shape[1] // 2
    half = tokens // 2

    def halves_of(shard):
        mine = lax.dynamic_slice_in_dim(shard, zl * units, units, 1)
        return mine, lax.dynamic_slice_in_dim(shard, (1 - zl) * units, units, 1)

    mine, theirs = halves_of(up_weight.astype(BF16))
    other = send(theirs, DOWNWARD)
    up_own = jnp.concatenate([jnp.where(zl == 0, mine, other), jnp.where(zl == 0, other, mine)], axis=0)

    mine, theirs = halves_of(down_weight.astype(BF16).T)
    lower = send(jnp.where(core == 0, theirs, mine), TO_LOWER)
    upper = send(jnp.where(core == 1, theirs, mine), TO_UPPER)
    ra, rb = jnp.where(core == 0, lower, upper), jnp.where(core == 0, upper, lower)
    down_own = jnp.concatenate([jnp.where(core == zl, mine, ra), jnp.where(core == zl, ra, rb)], axis=1)

    f32 = hidden_in.astype(jnp.float32)
    normed = (
        f32 * lax.rsqrt(jnp.mean(f32 * f32, axis=1, keepdims=True) + 1e-06) * norm_gain
    ).astype(BF16)
    held = jnp.concatenate([normed, send(normed[:half], UPWARD), send(normed[half:], DOWNWARD)], axis=0)
    others = send(held, SWAP)

    up_line = jnp.concatenate(around(up_own, FIRST), axis=0)
    up_plane = around(up_line, SECOND)
    down_line = jnp.concatenate(around(down_own, FIRST), axis=0)
    down_plane = around(down_line, SECOND)

    scale = lax.dynamic_slice_in_dim(up_scale, zl * units, units, 0).reshape(2, 1, units // 2)
    act = [up_call(part, pos, held, others, scale[part], up_plane) for part in range(2)]
    act += [send(h, SWAP) for h in act]

    gain = lax.dynamic_index_in_dim(down_scale.reshape(2, 4, 4, BLOCK), core, 0, keepdims=False)
    gain = jnp.where(core == 0, gain, jnp.swapaxes(gain, 0, 1)).reshape(4, LINE)
    gain = jnp.concatenate([lax.dynamic_slice_in_dim(gain, near(b, d), 1, 0) for d in NEAR], axis=1)
    mine, theirs = [], []
    for batch, refs in enumerate((down_plane[:3], down_plane[3:])):
        own, low, high = down_call(batch, pos, act, refs)
        above, below = send(low, DOWNWARD), send(high, UPWARD)
        start = batch * COLUMNS[0]
        kept, sent = sum_call(batch, pos, own, above, below, gain[:, start : start + COLUMNS[batch]])
        mine.append(kept)
        theirs.append(send(sent, SWAP))
    return last_call(pos, *mine, *theirs)


def solution(mesh):
    fine = Mesh(mesh.devices.reshape(2, 2, 4, 4, 2), AXES)
    fs = ("zl", "y", "x")
    rows = P(AXES, None)
    placed = (rows, P(), P(fs, "c"), P("c"), P("c", fs), P())
    return jax.shard_map(body, mesh=fine, in_specs=placed, out_specs=rows, check_vma=False)
```

```python
import functools

import jax
import jax.numpy as jnp
from jax import lax
from jax.experimental import pallas as pl
from jax.experimental.pallas import tpu as pltpu
from jax.sharding import Mesh, PartitionSpec as P


AXES = ("zh", "zl", "y", "x", "c")
NEAR = (0, -1, 1, 2)
BLOCK = 64
LINE = 4 * BLOCK
CHUNK = 512
STEP = 384
ANY = pl.BlockSpec(memory_space=pl.ANY)
SMEM = pl.BlockSpec(memory_space=pltpu.SMEM)
VMEM = pl.BlockSpec(memory_space=pltpu.VMEM)
BF16 = jnp.bfloat16


def index_of(z, y, x, c):
    return ((z % 4 * 4 + y % 4) * 4 + x % 4) * 2 + c


def pairs_of(target):
    pairs = []
    for z in range(4):
        for y in range(4):
            for x in range(4):
                for c in range(2):
                    to = target(z, y, x, c)
                    if to is not None:
                        pairs.append((index_of(z, y, x, c), index_of(*to)))
    return pairs


def first_ring(d):
    return pairs_of(lambda z, y, x, c: (z, y + d, x, c) if c else (z, y, x + d, c))


def second_ring(d):
    return pairs_of(lambda z, y, x, c: (z, y, x + d, c) if c else (z, y + d, x, c))


def z_ring(d):
    return pairs_of(lambda z, y, x, c: (z + d, y, x, c))


FIRST = (first_ring(1), first_ring(-1))
SECOND = (second_ring(1), second_ring(-1))
UPWARD, DOWNWARD = z_ring(1), z_ring(-1)
SWAP = pairs_of(lambda z, y, x, c: (z, y, x, 1 - c))


def to_lower(z, y, x, c):
    if c == 0:
        return z - 1, y, x, z % 2
    return (z, y, x, 0) if z % 2 == 0 else None


def to_upper(z, y, x, c):
    if c == 1:
        return z + 1, y, x, z % 2
    return (z, y, x, 1) if z % 2 == 1 else None


TO_LOWER, TO_UPPER = pairs_of(to_lower), pairs_of(to_upper)


def send(a, pairs):
    return lax.ppermute(a, AXES, pairs)


def first_line(own, ring):
    before, after = send(own, ring[0]), send(own, ring[1])
    n = own.shape[0] // 2
    far = send(before[:n], ring[0]), send(after[n:], ring[1])
    return jnp.concatenate([own, before], axis=0), jnp.concatenate([after, *far], axis=0)


def second_line(own, ring):
    low, high = own
    low_before, low_after = send(low, ring[0]), send(low, ring[1])
    high_before, high_after = send(high, ring[0]), send(high, ring[1])
    far = send(low_before, ring[0]), send(high_after, ring[1])
    return low, high, low_before, high_before, low_after, high_after, *far


def near(value, shift):
    return lax.rem(value + (shift + 4), 4)


def parts_of(refs):
    return [(ref, i, NEAR[k // 2], NEAR[k % 2 * 2 + i]) for k, ref in enumerate(refs) for i in range(2)]


def up_kernel(first, pos, x0, x1, scale, *refs):
    refs, (act, xv, wv, ov, xsem, wsem, osem) = refs[:8], refs[8:]
    a, b, sa, sb, core = pos[0], pos[1], pos[2], pos[3], pos[4]
    width, n = wv.shape
    held = x0.shape[0]
    chunks, steps = n // CHUNK, 2 * held // STEP

    def w_start(j):
        for ref, i, d, e in parts_of(refs):
            for level in range(2):
                at = pl.multiple_of(level * (width // 2) + near(a, e) * sa + near(b, d) * sb, BLOCK)
                pltpu.make_async_copy(
                    ref.at[pl.ds((2 * i + level) * BLOCK, BLOCK), pl.ds(first + j * CHUNK, CHUNK)],
                    wv.at[pl.ds(at, BLOCK), pl.ds(j * CHUNK, CHUNK)],
                    wsem.at[j],
                ).start()

    def x_copy(k):
        ref = x0 if k < steps // 2 else x1
        return pltpu.make_async_copy(ref.at[pl.ds(k * STEP % held, STEP)], xv.at[pl.ds(k * STEP, STEP)], xsem.at[k])

    w_start(0)
    for k in range(steps):
        x_copy(k).start()
    outs = []
    for j in range(chunks):
        cols = pl.ds(j * CHUNK, CHUNK)
        pltpu.make_async_copy(wv.at[:, cols], wv.at[:, cols], wsem.at[j]).wait()
        if j + 1 < chunks:
            w_start(j + 1)
        for side, who in ((0, core), (1, 1 - core)):

            def one(k, carry, side=side, who=who, cols=cols, j=j):
                src = pl.ds(pl.multiple_of(side * held + k * STEP, STEP), STEP)
                if j == 0:
                    pltpu.make_async_copy(xv.at[src], xv.at[src], xsem.at[side * (steps // 2) + k]).wait()
                dst = pl.ds(pl.multiple_of(who * held + k * STEP, STEP), STEP)
                pre = jnp.dot(xv[src, :], wv[:, cols], preferred_element_type=jnp.float32)
                pre = jnp.maximum(pre * scale[:, cols], 0.0)
                ov[dst, cols] = (pre * pre).astype(BF16)
                return carry

            lax.fori_loop(0, steps // 2, one, 0)
        out = pltpu.make_async_copy(ov.at[:, cols], act.at[:, cols], osem.at[j])
        out.start()
        outs.append(out)
    for out in outs:
        out.wait()


def up_call(part, pos, x0, x1, scale, weights):
    rows, width = 2 * x0.shape[0], x0.shape[1]
    n = scale.shape[1]
    return pl.pallas_call(
        functools.partial(up_kernel, part * n),
        out_shape=jax.ShapeDtypeStruct((rows, n), BF16),
        in_specs=[SMEM, ANY, ANY, VMEM] + [ANY] * 8,
        out_specs=ANY,
        scratch_shapes=[
            pltpu.VMEM((rows, width), BF16),
            pltpu.VMEM((width, n), BF16),
            pltpu.VMEM((rows, n), BF16),
            pltpu.SemaphoreType.DMA((rows // STEP,)),
            pltpu.SemaphoreType.DMA((n // CHUNK,)),
            pltpu.SemaphoreType.DMA((n // CHUNK,)),
        ],
        compiler_params=pltpu.CompilerParams(vmem_limit_bytes=22 * 2**20),
        cost_estimate=pl.CostEstimate(flops=2 * rows * width * n, bytes_accessed=2 * (rows * width + width * n + rows * n), transcendentals=0),
    )(pos, x0, x1, scale, *weights)


def down_kernel(pos, h0, h1, o0, o1, *refs):
    refs, (own, low, high, av, vv, ov, asem, vsem, osem) = refs[:-9], refs[-9:]
    a = pos[0]
    rows, quarter = h0.shape
    kept = rows // 4
    half = kept // 2

    def v_start(g):
        for k, ref in enumerate(refs[2 * g : 2 * g + 2]):
            for i in range(2):
                at = pl.multiple_of(g * LINE + near(a, NEAR[2 * k + i]) * BLOCK, BLOCK)
                pltpu.make_async_copy(ref.at[pl.ds(i * BLOCK, BLOCK)], vv.at[pl.ds(at, BLOCK)], vsem.at[g]).start()

    def a_copies(k):
        r = pl.ds(k * kept, kept)
        return [
            pltpu.make_async_copy(ref.at[r], av.at[r, pl.ds(q * quarter, quarter)], asem.at[4 * k + q])
            for q, ref in enumerate((h0, h1, o0, o1))
        ]

    groups = vv.shape[0] // LINE
    order = (1, 3, 0, 2)
    v_start(0)
    for copy in a_copies(order[0]):
        copy.start()
    for g in range(1, groups):
        v_start(g)
    for k in order[1:]:
        for copy in a_copies(k):
            copy.start()
    outs = []
    for k in order:
        for copy in a_copies(k):
            copy.wait()
        r = pl.ds(k * kept, kept)

        def one(g, carry, k=k, r=r):
            cols = pl.ds(pl.multiple_of(g * LINE, LINE), LINE)
            if k == order[0]:
                pltpu.make_async_copy(vv.at[cols], vv.at[cols], vsem.at[g]).wait()
            part = lax.dot_general(av[r, :], vv[cols, :], (((1,), (1,)), ((), ())), preferred_element_type=jnp.float32)
            ov[r, cols] = part.astype(BF16)
            return carry

        lax.fori_loop(0, groups, one, 0)
        c = k // 2
        if k % 2 == 0:
            moves = [(own, 0, kept)]
        else:
            moves = [(low, 0, half), (high, half, half)]
        for ref, start, size in moves:
            out = pltpu.make_async_copy(
                ov.at[pl.ds(k * kept + start, size)], ref.at[pl.ds(c * size, size)], osem.at[len(outs)]
            )
            out.start()
            outs.append(out)
    for out in outs:
        out.wait()


COLUMNS = (3 * LINE, LINE)


def down_call(batch, pos, act, refs):
    rows, units = act[0].shape[0], 4 * act[0].shape[1]
    n = COLUMNS[batch]
    return pl.pallas_call(
        down_kernel,
        out_shape=[jax.ShapeDtypeStruct((rows // k, n), BF16) for k in (2, 4, 4)],
        in_specs=[SMEM] + [ANY] * (4 + len(refs)),
        out_specs=[ANY] * 3,
        scratch_shapes=[
            pltpu.VMEM((rows, units), BF16),
            pltpu.VMEM((n, units), BF16),
            pltpu.VMEM((rows, n), BF16),
            pltpu.SemaphoreType.DMA((16,)),
            pltpu.SemaphoreType.DMA((n // LINE,)),
            pltpu.SemaphoreType.DMA((6,)),
        ],
        compiler_params=pltpu.CompilerParams(vmem_limit_bytes=(26, 20)[batch] * 2**20),
        cost_estimate=pl.CostEstimate(flops=2 * rows * units * n, bytes_accessed=2 * (rows * units + units * n + rows * n), transcendentals=0),
    )(pos, *act, *refs)


def sum_kernel(pos, own, above, below, gain, mine, theirs):
    core = pos[4]
    kept = mine.shape[0]
    half = kept // 2
    for ref, who in ((mine, core), (theirs, 1 - core)):
        for i, other in enumerate((above, below)):
            r = pl.ds(pl.multiple_of(who * kept + i * half, half), half)
            total = own[r, :].astype(jnp.float32) + other[pl.ds(pl.multiple_of(who * half, half), half), :].astype(jnp.float32)
            ref[pl.ds(i * half, half), :] = (total * gain[...]).astype(BF16)


def sum_call(pos, own, above, below, gain):
    shape = jax.ShapeDtypeStruct((own.shape[0] // 2, own.shape[1]), BF16)
    return pl.pallas_call(
        sum_kernel,
        out_shape=[shape, shape],
        in_specs=[SMEM, VMEM, VMEM, VMEM, VMEM],
        out_specs=[VMEM, VMEM],
        compiler_params=pltpu.CompilerParams(vmem_limit_bytes=6 * 2**20),
    )(pos, own, above, below, gain)


def last_kernel(pos, m0, m1, g0, g1, out, qv, ov, dsem, qsem, osem):
    core, y, x = pos[4], pos[5], pos[6]
    half = ov.shape[1]

    def pieces(wide, narrow):
        refs = ((wide, 0), (wide, 1), (wide, 2), (narrow, 0))
        return [(ref.at[:, pl.ds(i * LINE, LINE)], d) for (ref, i), d in zip(refs, NEAR)]

    def start(straight, mixed):
        for ref, d in straight:
            at = pl.multiple_of(near(y, d) * LINE, LINE)
            pltpu.make_async_copy(ref, out.at[:, pl.ds(at, LINE)], dsem.at[0]).start()
        for ref, d in mixed:
            pltpu.make_async_copy(ref, qv.at[near(x, d)], qsem.at[0]).start()

    @pl.when(core == 0)
    def _():
        start(pieces(m0, m1), pieces(g0, g1))

    @pl.when(core == 1)
    def _():
        start(pieces(g0, g1), pieces(m0, m1))

    pltpu.make_async_copy(qv, qv, qsem.at[0]).wait()
    left = lax.broadcasted_iota(jnp.int32, (qv.shape[1], 128), 1) < BLOCK
    for pair in range(2):
        for v in range(2):
            cols = pl.ds(128 * v, 128)
            even = qv[2 * pair, :, cols].astype(jnp.float32)
            odd = qv[2 * pair + 1, :, cols].astype(jnp.float32)
            ov[:, pl.ds(2 * v * LINE + pair * 128, 128)] = jnp.where(left, even, pltpu.roll(odd, BLOCK, 1)).astype(BF16)
            ov[:, pl.ds((2 * v + 1) * LINE + pair * 128, 128)] = jnp.where(left, pltpu.roll(even, BLOCK, 1), odd).astype(BF16)
    copy = pltpu.make_async_copy(ov, out.at[:, pl.ds(half, half)], osem.at[0])
    copy.start()
    copy.wait()
    pltpu.make_async_copy(ov, out.at[:, pl.ds(0, half)], dsem.at[0]).wait()


def last_call(pos, *refs):
    rows = refs[0].shape[0]
    return pl.pallas_call(
        last_kernel,
        name="last",
        out_shape=jax.ShapeDtypeStruct((rows, 8 * LINE), BF16),
        in_specs=[SMEM] + [ANY] * 4,
        out_specs=ANY,
        scratch_shapes=[
            pltpu.VMEM((4, rows, LINE), BF16),
            pltpu.VMEM((rows, 4 * LINE), BF16),
            pltpu.SemaphoreType.DMA((1,)),
            pltpu.SemaphoreType.DMA((1,)),
            pltpu.SemaphoreType.DMA((1,)),
        ],
        compiler_params=pltpu.CompilerParams(vmem_limit_bytes=6 * 2**20),
    )(pos, *refs)


def body(hidden_in, norm_gain, up_weight, up_scale, down_weight, down_scale):
    zl, y, x, core = (lax.axis_index(name) for name in ("zl", "y", "x", "c"))
    a, b = jnp.where(core == 0, x, y), jnp.where(core == 0, y, x)
    sa, sb = jnp.where(core == 0, BLOCK, LINE), jnp.where(core == 0, LINE, BLOCK)
    pos = jnp.stack([a, b, sa, sb, core, y, x]).astype(jnp.int32)
    tokens, _ = hidden_in.shape
    units = up_weight.shape[1] // 2
    half = tokens // 2

    def halves_of(shard):
        mine = lax.dynamic_slice_in_dim(shard, zl * units, units, 1)
        return mine, lax.dynamic_slice_in_dim(shard, (1 - zl) * units, units, 1)

    mine, theirs = halves_of(up_weight.astype(BF16))
    other = send(theirs, DOWNWARD)
    up_own = jnp.concatenate([jnp.where(zl == 0, mine, other), jnp.where(zl == 0, other, mine)], axis=0)

    mine, theirs = halves_of(down_weight.astype(BF16).T)
    lower = send(jnp.where(core == 0, theirs, mine), TO_LOWER)
    upper = send(jnp.where(core == 1, theirs, mine), TO_UPPER)
    ra, rb = jnp.where(core == 0, lower, upper), jnp.where(core == 0, upper, lower)
    down_own = jnp.concatenate([jnp.where(core == zl, mine, ra), jnp.where(core == zl, ra, rb)], axis=1)

    f32 = hidden_in.astype(jnp.float32)
    normed = (
        f32 * lax.rsqrt(jnp.mean(f32 * f32, axis=1, keepdims=True) + 1e-06) * norm_gain
    ).astype(BF16)
    held = jnp.concatenate([normed, send(normed[:half], UPWARD), send(normed[half:], DOWNWARD)], axis=0)
    others = send(held, SWAP)

    up_plane = second_line(first_line(up_own, FIRST), SECOND)
    down_plane = second_line(first_line(down_own, FIRST), SECOND)

    scale = lax.dynamic_slice_in_dim(up_scale, zl * units, units, 0).reshape(2, 1, units // 2)
    act = [up_call(part, pos, held, others, scale[part], up_plane) for part in range(2)]
    act += [send(h, SWAP) for h in act]

    gain = lax.dynamic_index_in_dim(down_scale.reshape(2, 4, 4, BLOCK), core, 0, keepdims=False)
    gain = jnp.where(core == 0, gain, jnp.swapaxes(gain, 0, 1)).reshape(4, LINE)
    gain = jnp.concatenate([lax.dynamic_slice_in_dim(gain, near(b, d), 1, 0) for d in NEAR], axis=1)
    mine, theirs = [], []
    for batch, refs in enumerate((down_plane[:6], down_plane[6:])):
        own, low, high = down_call(batch, pos, act, refs)
        above, below = send(low, DOWNWARD), send(high, UPWARD)
        start = batch * COLUMNS[0]
        kept, sent = sum_call(pos, own, above, below, gain[:, start : start + COLUMNS[batch]])
        mine.append(kept)
        theirs.append(send(sent, SWAP))
    return last_call(pos, *mine, *theirs)


def solution(mesh):
    fine = Mesh(mesh.devices.reshape(2, 2, 4, 4, 2), AXES)
    fs = ("zl", "y", "x")
    rows = P(AXES, None)
    placed = (rows, P(), P(fs, "c"), P("c"), P("c", fs), P())
    return jax.shard_map(body, mesh=fine, in_specs=placed, out_specs=rows, check_vma=False)
```

```python
import functools

import jax
import jax.numpy as jnp
from jax import lax
from jax.experimental import pallas as pl
from jax.experimental.pallas import tpu as pltpu
from jax.sharding import Mesh, PartitionSpec as P


AXES = ("zh", "zl", "y", "x", "c")
NEAR = (0, -1, 1, 2)
BLOCK = 64
LINE = 4 * BLOCK
CHUNK = 512
STEP = 384
COLUMNS = (3 * LINE, LINE)
ANY = pl.BlockSpec(memory_space=pl.ANY)
SMEM = pl.BlockSpec(memory_space=pltpu.SMEM)
VMEM = pl.BlockSpec(memory_space=pltpu.VMEM)
BF16 = jnp.bfloat16


def index_of(z, y, x, c):
    return ((z % 4 * 4 + y % 4) * 4 + x % 4) * 2 + c


def pairs_of(target):
    pairs = []
    for z in range(4):
        for y in range(4):
            for x in range(4):
                for c in range(2):
                    to = target(z, y, x, c)
                    if to is not None:
                        pairs.append((index_of(z, y, x, c), index_of(*to)))
    return pairs


def first_ring(d):
    return pairs_of(lambda z, y, x, c: (z, y + d, x, c) if c else (z, y, x + d, c))


def second_ring(d):
    return pairs_of(lambda z, y, x, c: (z, y, x + d, c) if c else (z, y + d, x, c))


def z_ring(d):
    return pairs_of(lambda z, y, x, c: (z + d, y, x, c))


FIRST = (first_ring(1), first_ring(-1))
SECOND = (second_ring(1), second_ring(-1))
UPWARD, DOWNWARD = z_ring(1), z_ring(-1)
SWAP = pairs_of(lambda z, y, x, c: (z, y, x, 1 - c))


def to_lower(z, y, x, c):
    if c == 0:
        return z - 1, y, x, z % 2
    return (z, y, x, 0) if z % 2 == 0 else None


def to_upper(z, y, x, c):
    if c == 1:
        return z + 1, y, x, z % 2
    return (z, y, x, 1) if z % 2 == 1 else None


TO_LOWER, TO_UPPER = pairs_of(to_lower), pairs_of(to_upper)


def send(a, pairs):
    return lax.ppermute(a, AXES, pairs)


def first_line(own, ring):
    before, after = send(own, ring[0]), send(own, ring[1])
    n = own.shape[0] // 2
    far = send(before[:n], ring[0]), send(after[n:], ring[1])
    return jnp.concatenate([own, before], axis=0), jnp.concatenate([after, *far], axis=0)


def second_line(own, ring):
    low, high = own
    low_before, low_after = send(low, ring[0]), send(low, ring[1])
    high_before, high_after = send(high, ring[0]), send(high, ring[1])
    far = send(low_before, ring[0]), send(high_after, ring[1])
    return low, high, low_before, high_before, low_after, high_after, *far


def near(value, shift):
    return lax.rem(value + (shift + 4), 4)


def parts_of(refs):
    return [(ref, i, NEAR[k // 2], NEAR[k % 2 * 2 + i]) for k, ref in enumerate(refs) for i in range(2)]


def up_kernel(first, pos, x0, x1, scale, *refs):
    refs, (act, wv, wsem) = refs[:8], refs[8:]
    a, b, sa, sb, core = pos[0], pos[1], pos[2], pos[3], pos[4]
    width, n = wv.shape
    held = x0.shape[0]
    chunks = n // CHUNK

    def w_start(j):
        for ref, i, d, e in parts_of(refs):
            for level in range(2):
                at = pl.multiple_of(level * (width // 2) + near(a, e) * sa + near(b, d) * sb, BLOCK)
                pltpu.make_async_copy(
                    ref.at[pl.ds((2 * i + level) * BLOCK, BLOCK), pl.ds(first + j * CHUNK, CHUNK)],
                    wv.at[pl.ds(at, BLOCK), pl.ds(j * CHUNK, CHUNK)],
                    wsem.at[j],
                ).start()

    def w_wait(j):
        cols = pl.ds(pl.multiple_of(j * CHUNK, CHUNK), CHUNK)
        pltpu.make_async_copy(wv.at[:, cols], wv.at[:, cols], wsem.at[j]).wait()

    w_start(0)
    w_wait(0)
    w_start(1)

    def chunk(j, carry):
        cols = pl.ds(pl.multiple_of(j * CHUNK, CHUNK), CHUNK)

        @pl.when(j > 0)
        def _():
            w_wait(j)

        for ref, who in ((x0, core), (x1, 1 - core)):

            def one(k, carry, ref=ref, who=who):
                src = pl.ds(pl.multiple_of(k * STEP, STEP), STEP)
                dst = pl.ds(pl.multiple_of(who * held + k * STEP, STEP), STEP)
                pre = jnp.dot(ref[src, :], wv[:, cols], preferred_element_type=jnp.float32)
                pre = jnp.maximum(pre * scale[:, cols], 0.0)
                act[dst, cols] = (pre * pre).astype(BF16)
                return carry

            lax.fori_loop(0, held // STEP, one, 0)
        return carry

    lax.fori_loop(0, chunks, chunk, 0)


def up_call(part, pos, x0, x1, scale, weights):
    rows, width = 2 * x0.shape[0], x0.shape[1]
    n = scale.shape[1]
    return pl.pallas_call(
        functools.partial(up_kernel, part * n),
        out_shape=jax.ShapeDtypeStruct((rows, n), BF16),
        in_specs=[SMEM, VMEM, VMEM, VMEM] + [ANY] * 8,
        out_specs=VMEM,
        scratch_shapes=[
            pltpu.VMEM((width, n), BF16),
            pltpu.SemaphoreType.DMA((n // CHUNK,)),
        ],
        compiler_params=pltpu.CompilerParams(vmem_limit_bytes=14 * 2**20),
        cost_estimate=pl.CostEstimate(flops=2 * rows * width * n, bytes_accessed=2 * (rows * width + width * n + rows * n), transcendentals=0),
    )(pos, x0, x1, scale, *weights)


def down_kernel(pos, h0, h1, o0, o1, *refs):
    refs, (own, low, high, vv, ov, vsem, osem) = refs[:-7], refs[-7:]
    a = pos[0]
    rows, quarter = h0.shape
    kept = rows // 4
    half = kept // 2

    def v_start(g):
        for k, ref in enumerate(refs[2 * g : 2 * g + 2]):
            for i in range(4):
                at = pl.multiple_of(g * LINE + near(a, NEAR[2 * k + i // 2]) * BLOCK, BLOCK)
                pltpu.make_async_copy(
                    ref.at[pl.ds(i * BLOCK, BLOCK)],
                    vv.at[pl.ds(at, BLOCK), pl.ds(i % 2 * 2 * quarter, 2 * quarter)],
                    vsem.at[g],
                ).start()

    groups = vv.shape[0] // LINE
    for g in range(groups):
        v_start(g)

    def out_copies(c):
        rows_of = ((own, 0, kept), (low, kept, half), (high, kept + half, half))
        return [
            pltpu.make_async_copy(
                ov.at[pl.ds(c * 2 * kept + start, size)], ref.at[pl.ds(c * size, size)], osem.at[3 * c + i]
            )
            for i, (ref, start, size) in enumerate(rows_of)
        ]

    def chunk(k, carry):
        r = pl.ds(pl.multiple_of(k * kept, kept), kept)

        def one(g, carry):
            cols = pl.ds(pl.multiple_of(g * LINE, LINE), LINE)

            @pl.when(k == 0)
            def _():
                pltpu.make_async_copy(vv.at[cols], vv.at[cols], vsem.at[g]).wait()

            part = None
            for q, ref in enumerate((h0, h1, o0, o1)):
                term = lax.dot_general(
                    ref[r, :],
                    vv[cols, pl.ds(q * quarter, quarter)],
                    (((1,), (1,)), ((), ())),
                    preferred_element_type=jnp.float32,
                )
                part = term if part is None else part + term
            ov[r, cols] = part.astype(BF16)
            return carry

        lax.fori_loop(0, groups, one, 0)
        for c in range(2):
            own_copy, *z_copies = out_copies(c)

            @pl.when(k == 2 * c)
            def _():
                own_copy.start()

            @pl.when(k == 2 * c + 1)
            def _():
                for copy in z_copies:
                    copy.start()

        return carry

    lax.fori_loop(0, 4, chunk, 0)
    for c in range(2):
        for copy in out_copies(c):
            copy.wait()


def down_call(batch, pos, act, refs):
    rows, units = act[0].shape[0], 4 * act[0].shape[1]
    n = COLUMNS[batch]
    return pl.pallas_call(
        down_kernel,
        out_shape=[jax.ShapeDtypeStruct((rows // k, n), BF16) for k in (2, 4, 4)],
        in_specs=[SMEM] + [VMEM] * 4 + [ANY] * len(refs),
        out_specs=[ANY] * 3,
        scratch_shapes=[
            pltpu.VMEM((n, units), BF16),
            pltpu.VMEM((rows, n), BF16),
            pltpu.SemaphoreType.DMA((n // LINE,)),
            pltpu.SemaphoreType.DMA((6,)),
        ],
        compiler_params=pltpu.CompilerParams(vmem_limit_bytes=(16, 10)[batch] * 2**20),
        cost_estimate=pl.CostEstimate(flops=2 * rows * units * n, bytes_accessed=2 * (rows * units + units * n + rows * n), transcendentals=0),
    )(pos, *act, *refs)


def sum_kernel(pos, own, above, below, gain, mine, theirs):
    core = pos[4]
    kept = mine.shape[0]
    half = kept // 2
    for ref, who in ((mine, core), (theirs, 1 - core)):
        for i, other in enumerate((above, below)):
            r = pl.ds(pl.multiple_of(who * kept + i * half, half), half)
            total = own[r, :].astype(jnp.float32) + other[pl.ds(pl.multiple_of(who * half, half), half), :].astype(jnp.float32)
            ref[pl.ds(i * half, half), :] = (total * gain[...]).astype(BF16)


def sum_call(pos, own, above, below, gain):
    shape = jax.ShapeDtypeStruct((own.shape[0] // 2, own.shape[1]), BF16)
    return pl.pallas_call(
        sum_kernel,
        out_shape=[shape, shape],
        in_specs=[SMEM, VMEM, VMEM, VMEM, VMEM],
        out_specs=[VMEM, VMEM],
        compiler_params=pltpu.CompilerParams(vmem_limit_bytes=6 * 2**20),
    )(pos, own, above, below, gain)


def last_kernel(pos, m0, m1, g0, g1, out, qv, ov, dsem, qsem, osem):
    core, y, x = pos[4], pos[5], pos[6]
    half = ov.shape[1]

    def pieces(wide, narrow):
        refs = ((wide, 0), (wide, 1), (wide, 2), (narrow, 0))
        return [(ref.at[:, pl.ds(i * LINE, LINE)], d) for (ref, i), d in zip(refs, NEAR)]

    def start(straight, mixed):
        for ref, d in straight:
            at = pl.multiple_of(near(y, d) * LINE, LINE)
            pltpu.make_async_copy(ref, out.at[:, pl.ds(at, LINE)], dsem.at[0]).start()
        for ref, d in mixed:
            pltpu.make_async_copy(ref, qv.at[near(x, d)], qsem.at[0]).start()

    @pl.when(core == 0)
    def _():
        start(pieces(m0, m1), pieces(g0, g1))

    @pl.when(core == 1)
    def _():
        start(pieces(g0, g1), pieces(m0, m1))

    pltpu.make_async_copy(qv, qv, qsem.at[0]).wait()
    left = lax.broadcasted_iota(jnp.int32, (qv.shape[1], 128), 1) < BLOCK
    for pair in range(2):
        for v in range(2):
            cols = pl.ds(128 * v, 128)
            even = qv[2 * pair, :, cols].astype(jnp.float32)
            odd = qv[2 * pair + 1, :, cols].astype(jnp.float32)
            ov[:, pl.ds(2 * v * LINE + pair * 128, 128)] = jnp.where(left, even, pltpu.roll(odd, BLOCK, 1)).astype(BF16)
            ov[:, pl.ds((2 * v + 1) * LINE + pair * 128, 128)] = jnp.where(left, pltpu.roll(even, BLOCK, 1), odd).astype(BF16)
    copy = pltpu.make_async_copy(ov, out.at[:, pl.ds(half, half)], osem.at[0])
    copy.start()
    copy.wait()
    pltpu.make_async_copy(ov, out.at[:, pl.ds(0, half)], dsem.at[0]).wait()


def last_call(pos, *refs):
    rows = refs[0].shape[0]
    return pl.pallas_call(
        last_kernel,
        name="last",
        out_shape=jax.ShapeDtypeStruct((rows, 8 * LINE), BF16),
        in_specs=[SMEM] + [ANY] * 4,
        out_specs=ANY,
        scratch_shapes=[
            pltpu.VMEM((4, rows, LINE), BF16),
            pltpu.VMEM((rows, 4 * LINE), BF16),
            pltpu.SemaphoreType.DMA((1,)),
            pltpu.SemaphoreType.DMA((1,)),
            pltpu.SemaphoreType.DMA((1,)),
        ],
        compiler_params=pltpu.CompilerParams(vmem_limit_bytes=6 * 2**20),
    )(pos, *refs)


def body(hidden_in, norm_gain, up_weight, up_scale, down_weight, down_scale):
    zl, y, x, core = (lax.axis_index(name) for name in ("zl", "y", "x", "c"))
    a, b = jnp.where(core == 0, x, y), jnp.where(core == 0, y, x)
    sa, sb = jnp.where(core == 0, BLOCK, LINE), jnp.where(core == 0, LINE, BLOCK)
    pos = jnp.stack([a, b, sa, sb, core, y, x]).astype(jnp.int32)
    tokens, _ = hidden_in.shape
    units = up_weight.shape[1] // 2
    half = tokens // 2

    def halves_of(shard):
        mine = lax.dynamic_slice_in_dim(shard, zl * units, units, 1)
        return mine, lax.dynamic_slice_in_dim(shard, (1 - zl) * units, units, 1)

    mine, theirs = halves_of(up_weight.astype(BF16))
    other = send(theirs, DOWNWARD)
    up_own = [jnp.where(zl == 0, mine, other), jnp.where(zl == 0, other, mine)]

    mine, theirs = halves_of(down_weight.astype(BF16).T)
    lower = send(jnp.where(core == 0, theirs, mine), TO_LOWER)
    upper = send(jnp.where(core == 1, theirs, mine), TO_UPPER)
    ra, rb = jnp.where(core == 0, lower, upper), jnp.where(core == 0, upper, lower)
    down_own = [jnp.where(core == zl, mine, ra), jnp.where(core == zl, ra, rb)]

    f32 = hidden_in.astype(jnp.float32)
    normed = (
        f32 * lax.rsqrt(jnp.mean(f32 * f32, axis=1, keepdims=True) + 1e-06) * norm_gain
    ).astype(BF16)
    held = jnp.concatenate([normed, send(normed[:half], UPWARD), send(normed[half:], DOWNWARD)], axis=0)
    scale = lax.dynamic_slice_in_dim(up_scale, zl * units, units, 0).reshape(2, 1, units // 2)
    gain = lax.dynamic_index_in_dim(down_scale.reshape(2, 4, 4, BLOCK), core, 0, keepdims=False)
    gain = jnp.where(core == 0, gain, jnp.swapaxes(gain, 0, 1)).reshape(4, LINE)
    gain = jnp.concatenate([lax.dynamic_slice_in_dim(gain, near(b, d), 1, 0) for d in NEAR], axis=1)
    tables = [gain[:, : COLUMNS[0]], gain[:, COLUMNS[0] :]]
    held, pos, scale0, scale1, *tables = lax.optimization_barrier((held, pos, scale[0], scale[1], *tables))
    scale = (scale0, scale1)
    others = send(held, SWAP)

    up_plane = second_line(first_line(jnp.concatenate(up_own, axis=0), FIRST), SECOND)
    down_plane = second_line(first_line(jnp.concatenate(down_own, axis=0), FIRST), SECOND)

    act = [up_call(part, pos, held, others, scale[part], up_plane) for part in range(2)]
    act += [send(h, SWAP) for h in act]

    mine, theirs = [], []
    for batch, refs in enumerate((down_plane[:6], down_plane[6:])):
        own, low, high = down_call(batch, pos, act, refs)
        above, below = send(low, DOWNWARD), send(high, UPWARD)
        kept, sent = sum_call(pos, own, above, below, tables[batch])
        mine.append(kept)
        theirs.append(send(sent, SWAP))
    return last_call(pos, *mine, *theirs)


def solution(mesh):
    fine = Mesh(mesh.devices.reshape(2, 2, 4, 4, 2), AXES)
    fs = ("zl", "y", "x")
    rows = P(AXES, None)
    placed = (rows, P(), P(fs, "c"), P("c"), P("c", fs), P())
    return jax.shard_map(body, mesh=fine, in_specs=placed, out_specs=rows, check_vma=False)
```

```python
import functools

import jax
import jax.numpy as jnp
from jax import lax
from jax.experimental import pallas as pl
from jax.experimental.pallas import tpu as pltpu
from jax.sharding import Mesh, PartitionSpec as P


AXES = ("zh", "zl", "y", "x", "c")
NEAR = (0, -1, 1, 2)
BLOCK = 64
LINE = 4 * BLOCK
CHUNK = 512
STEP = 384
COLUMNS = (2 * LINE, 2 * LINE)
ANY = pl.BlockSpec(memory_space=pl.ANY)
SMEM = pl.BlockSpec(memory_space=pltpu.SMEM)
VMEM = pl.BlockSpec(memory_space=pltpu.VMEM)
BF16 = jnp.bfloat16


def index_of(z, y, x, c):
    return ((z % 4 * 4 + y % 4) * 4 + x % 4) * 2 + c


def pairs_of(target):
    pairs = []
    for z in range(4):
        for y in range(4):
            for x in range(4):
                for c in range(2):
                    to = target(z, y, x, c)
                    if to is not None:
                        pairs.append((index_of(z, y, x, c), index_of(*to)))
    return pairs


def first_ring(d):
    return pairs_of(lambda z, y, x, c: (z, y + d, x, c) if c else (z, y, x + d, c))


def second_ring(d):
    return pairs_of(lambda z, y, x, c: (z, y, x + d, c) if c else (z, y + d, x, c))


def z_ring(d):
    return pairs_of(lambda z, y, x, c: (z + d, y, x, c))


FIRST = (first_ring(1), first_ring(-1))
SECOND = (second_ring(1), second_ring(-1))
UPWARD, DOWNWARD = z_ring(1), z_ring(-1)
SWAP = pairs_of(lambda z, y, x, c: (z, y, x, 1 - c))


def to_lower(z, y, x, c):
    if c == 0:
        return z - 1, y, x, z % 2
    return (z, y, x, 0) if z % 2 == 0 else None


def to_upper(z, y, x, c):
    if c == 1:
        return z + 1, y, x, z % 2
    return (z, y, x, 1) if z % 2 == 1 else None


TO_LOWER, TO_UPPER = pairs_of(to_lower), pairs_of(to_upper)


def send(a, pairs):
    return lax.ppermute(a, AXES, pairs)


def first_line(own, ring):
    before, after = send(own, ring[0]), send(own, ring[1])
    n = own.shape[0] // 2
    far = send(before[:n], ring[0]), send(after[n:], ring[1])
    return jnp.concatenate([own, before], axis=0), jnp.concatenate([after, *far], axis=0)


def second_line(own, ring):
    low, high = own
    low_before, low_after = send(low, ring[0]), send(low, ring[1])
    high_before, high_after = send(high, ring[0]), send(high, ring[1])
    far = send(low_before, ring[0]), send(high_after, ring[1])
    return low, high, low_before, high_before, low_after, high_after, *far


def near(value, shift):
    return lax.rem(value + (shift + 4), 4)


def parts_of(refs):
    return [(ref, i, NEAR[k // 2], NEAR[k % 2 * 2 + i]) for k, ref in enumerate(refs) for i in range(2)]


def up_kernel(first, pos, x0, x1, scale, *refs):
    refs, (act, wv, wsem) = refs[:8], refs[8:]
    a, b, sa, sb, core = pos[0], pos[1], pos[2], pos[3], pos[4]
    width, n = wv.shape
    held = x0.shape[0]
    chunks = n // CHUNK

    def w_start(j):
        for ref, i, d, e in parts_of(refs):
            for level in range(2):
                at = pl.multiple_of(level * (width // 2) + near(a, e) * sa + near(b, d) * sb, BLOCK)
                pltpu.make_async_copy(
                    ref.at[pl.ds((2 * i + level) * BLOCK, BLOCK), pl.ds(first + j * CHUNK, CHUNK)],
                    wv.at[pl.ds(at, BLOCK), pl.ds(j * CHUNK, CHUNK)],
                    wsem.at[j],
                ).start()

    def w_wait(j):
        cols = pl.ds(pl.multiple_of(j * CHUNK, CHUNK), CHUNK)
        pltpu.make_async_copy(wv.at[:, cols], wv.at[:, cols], wsem.at[j]).wait()

    w_start(0)
    w_wait(0)
    w_start(1)

    def chunk(j, carry):
        cols = pl.ds(pl.multiple_of(j * CHUNK, CHUNK), CHUNK)

        @pl.when(j > 0)
        def _():
            w_wait(j)

        for ref, who in ((x0, core), (x1, 1 - core)):

            def one(k, carry, ref=ref, who=who):
                src = pl.ds(pl.multiple_of(k * STEP, STEP), STEP)
                dst = pl.ds(pl.multiple_of(who * held + k * STEP, STEP), STEP)
                pre = jnp.dot(ref[src, :], wv[:, cols], preferred_element_type=jnp.float32)
                pre = jnp.maximum(pre * scale[:, cols], 0.0)
                act[dst, cols] = (pre * pre).astype(BF16)
                return carry

            lax.fori_loop(0, held // STEP, one, 0)
        return carry

    lax.fori_loop(0, chunks, chunk, 0)


def up_call(part, pos, x0, x1, scale, weights):
    rows, width = 2 * x0.shape[0], x0.shape[1]
    n = scale.shape[1]
    return pl.pallas_call(
        functools.partial(up_kernel, part * n),
        out_shape=jax.ShapeDtypeStruct((rows, n), BF16),
        in_specs=[SMEM, VMEM, VMEM, VMEM] + [ANY] * 8,
        out_specs=VMEM,
        scratch_shapes=[
            pltpu.VMEM((width, n), BF16),
            pltpu.SemaphoreType.DMA((n // CHUNK,)),
        ],
        compiler_params=pltpu.CompilerParams(vmem_limit_bytes=14 * 2**20),
        cost_estimate=pl.CostEstimate(flops=2 * rows * width * n, bytes_accessed=2 * (rows * width + width * n + rows * n), transcendentals=0),
    )(pos, x0, x1, scale, *weights)


def down_kernel(pos, h0, h1, o0, o1, *refs):
    refs, (own, low, high, vv, ov, vsem, osem) = refs[:-7], refs[-7:]
    a = pos[0]
    rows, quarter = h0.shape
    kept = rows // 4
    half = kept // 2

    def v_start(g):
        for k, ref in enumerate(refs[2 * g : 2 * g + 2]):
            for i in range(4):
                at = pl.multiple_of(g * LINE + near(a, NEAR[2 * k + i // 2]) * BLOCK, BLOCK)
                pltpu.make_async_copy(
                    ref.at[pl.ds(i * BLOCK, BLOCK)],
                    vv.at[pl.ds(at, BLOCK), pl.ds(i % 2 * 2 * quarter, 2 * quarter)],
                    vsem.at[g],
                ).start()

    groups = vv.shape[0] // LINE
    for g in range(groups):
        v_start(g)

    def out_copies(c):
        rows_of = ((own, 0, kept), (low, kept, half), (high, kept + half, half))
        return [
            pltpu.make_async_copy(
                ov.at[pl.ds(c * 2 * kept + start, size)], ref.at[pl.ds(c * size, size)], osem.at[3 * c + i]
            )
            for i, (ref, start, size) in enumerate(rows_of)
        ]

    def chunk(k, carry):
        r = pl.ds(pl.multiple_of(k * 2 * kept, 2 * kept), 2 * kept)

        def one(g, carry):
            cols = pl.ds(pl.multiple_of(g * LINE, LINE), LINE)

            @pl.when(k == 0)
            def _():
                pltpu.make_async_copy(vv.at[cols], vv.at[cols], vsem.at[g]).wait()

            part = None
            for q, ref in enumerate((h0, h1, o0, o1)):
                term = lax.dot_general(
                    ref[r, :],
                    vv[cols, pl.ds(q * quarter, quarter)],
                    (((1,), (1,)), ((), ())),
                    preferred_element_type=jnp.float32,
                )
                part = term if part is None else part + term
            ov[r, cols] = part.astype(BF16)
            return carry

        lax.fori_loop(0, groups, one, 0)
        for c in range(2):

            @pl.when(k == c)
            def _():
                for copy in out_copies(c):
                    copy.start()

        return carry

    lax.fori_loop(0, 2, chunk, 0)
    for c in range(2):
        for copy in out_copies(c):
            copy.wait()


def down_call(batch, pos, act, refs):
    rows, units = act[0].shape[0], 4 * act[0].shape[1]
    n = COLUMNS[batch]
    return pl.pallas_call(
        down_kernel,
        out_shape=[jax.ShapeDtypeStruct((rows // k, n), BF16) for k in (2, 4, 4)],
        in_specs=[SMEM] + [VMEM] * 4 + [ANY] * len(refs),
        out_specs=[ANY] * 3,
        scratch_shapes=[
            pltpu.VMEM((n, units), BF16),
            pltpu.VMEM((rows, n), BF16),
            pltpu.SemaphoreType.DMA((n // LINE,)),
            pltpu.SemaphoreType.DMA((6,)),
        ],
        compiler_params=pltpu.CompilerParams(vmem_limit_bytes=14 * 2**20),
        cost_estimate=pl.CostEstimate(flops=2 * rows * units * n, bytes_accessed=2 * (rows * units + units * n + rows * n), transcendentals=0),
    )(pos, *act, *refs)


def sum_kernel(pos, own, above, below, gain, mine, theirs):
    core = pos[4]
    kept = mine.shape[0]
    half = kept // 2
    for ref, who in ((mine, core), (theirs, 1 - core)):
        for i, other in enumerate((above, below)):
            r = pl.ds(pl.multiple_of(who * kept + i * half, half), half)
            total = own[r, :].astype(jnp.float32) + other[pl.ds(pl.multiple_of(who * half, half), half), :].astype(jnp.float32)
            ref[pl.ds(i * half, half), :] = (total * gain[...]).astype(BF16)


def sum_call(pos, own, above, below, gain):
    shape = jax.ShapeDtypeStruct((own.shape[0] // 2, own.shape[1]), BF16)
    return pl.pallas_call(
        sum_kernel,
        out_shape=[shape, shape],
        in_specs=[SMEM, VMEM, VMEM, VMEM, VMEM],
        out_specs=[VMEM, VMEM],
        compiler_params=pltpu.CompilerParams(vmem_limit_bytes=6 * 2**20),
    )(pos, own, above, below, gain)


def last_kernel(pos, m0, m1, g0, g1, out, qv, ov, dsem, qsem, osem):
    core, y, x = pos[4], pos[5], pos[6]
    half = ov.shape[1]

    def pieces(near_two, far_two):
        refs = ((near_two, 0), (near_two, 1), (far_two, 0), (far_two, 1))
        return [(ref.at[:, pl.ds(i * LINE, LINE)], d) for (ref, i), d in zip(refs, NEAR)]

    def start(straight, mixed):
        for ref, d in straight:
            at = pl.multiple_of(near(y, d) * LINE, LINE)
            pltpu.make_async_copy(ref, out.at[:, pl.ds(at, LINE)], dsem.at[0]).start()
        for ref, d in mixed:
            pltpu.make_async_copy(ref, qv.at[near(x, d)], qsem.at[0]).start()

    @pl.when(core == 0)
    def _():
        start(pieces(m0, m1), pieces(g0, g1))

    @pl.when(core == 1)
    def _():
        start(pieces(g0, g1), pieces(m0, m1))

    pltpu.make_async_copy(qv, qv, qsem.at[0]).wait()
    left = lax.broadcasted_iota(jnp.int32, (qv.shape[1], 128), 1) < BLOCK
    for pair in range(2):
        for v in range(2):
            cols = pl.ds(128 * v, 128)
            even = qv[2 * pair, :, cols].astype(jnp.float32)
            odd = qv[2 * pair + 1, :, cols].astype(jnp.float32)
            ov[:, pl.ds(2 * v * LINE + pair * 128, 128)] = jnp.where(left, even, pltpu.roll(odd, BLOCK, 1)).astype(BF16)
            ov[:, pl.ds((2 * v + 1) * LINE + pair * 128, 128)] = jnp.where(left, pltpu.roll(even, BLOCK, 1), odd).astype(BF16)
    copy = pltpu.make_async_copy(ov, out.at[:, pl.ds(half, half)], osem.at[0])
    copy.start()
    copy.wait()
    pltpu.make_async_copy(ov, out.at[:, pl.ds(0, half)], dsem.at[0]).wait()


def last_call(pos, *refs):
    rows = refs[0].shape[0]
    return pl.pallas_call(
        last_kernel,
        name="last",
        out_shape=jax.ShapeDtypeStruct((rows, 8 * LINE), BF16),
        in_specs=[SMEM] + [ANY] * 4,
        out_specs=ANY,
        scratch_shapes=[
            pltpu.VMEM((4, rows, LINE), BF16),
            pltpu.VMEM((rows, 4 * LINE), BF16),
            pltpu.SemaphoreType.DMA((1,)),
            pltpu.SemaphoreType.DMA((1,)),
            pltpu.SemaphoreType.DMA((1,)),
        ],
        compiler_params=pltpu.CompilerParams(vmem_limit_bytes=6 * 2**20),
    )(pos, *refs)


def body(hidden_in, norm_gain, up_weight, up_scale, down_weight, down_scale):
    zl, y, x, core = (lax.axis_index(name) for name in ("zl", "y", "x", "c"))
    a, b = jnp.where(core == 0, x, y), jnp.where(core == 0, y, x)
    sa, sb = jnp.where(core == 0, BLOCK, LINE), jnp.where(core == 0, LINE, BLOCK)
    pos = jnp.stack([a, b, sa, sb, core, y, x]).astype(jnp.int32)
    tokens, _ = hidden_in.shape
    units = up_weight.shape[1] // 2
    half = tokens // 2

    def halves_of(shard):
        mine = lax.dynamic_slice_in_dim(shard, zl * units, units, 1)
        return mine, lax.dynamic_slice_in_dim(shard, (1 - zl) * units, units, 1)

    mine, theirs = halves_of(up_weight.astype(BF16))
    other = send(theirs, DOWNWARD)
    up_own = [jnp.where(zl == 0, mine, other), jnp.where(zl == 0, other, mine)]

    mine, theirs = halves_of(down_weight.astype(BF16).T)
    lower = send(jnp.where(core == 0, theirs, mine), TO_LOWER)
    upper = send(jnp.where(core == 1, theirs, mine), TO_UPPER)
    ra, rb = jnp.where(core == 0, lower, upper), jnp.where(core == 0, upper, lower)
    down_own = [jnp.where(core == zl, mine, ra), jnp.where(core == zl, ra, rb)]

    f32 = hidden_in.astype(jnp.float32)
    normed = (
        f32 * lax.rsqrt(jnp.mean(f32 * f32, axis=1, keepdims=True) + 1e-06) * norm_gain
    ).astype(BF16)
    held = jnp.concatenate([normed, send(normed[:half], UPWARD), send(normed[half:], DOWNWARD)], axis=0)
    scale = lax.dynamic_slice_in_dim(up_scale, zl * units, units, 0).reshape(2, 1, units // 2)
    gain = lax.dynamic_index_in_dim(down_scale.reshape(2, 4, 4, BLOCK), core, 0, keepdims=False)
    gain = jnp.where(core == 0, gain, jnp.swapaxes(gain, 0, 1)).reshape(4, LINE)
    gain = jnp.concatenate([lax.dynamic_slice_in_dim(gain, near(b, d), 1, 0) for d in NEAR], axis=1)
    tables = [gain[:, : COLUMNS[0]], gain[:, COLUMNS[0] :]]
    held, pos, scale0, scale1, *tables = lax.optimization_barrier((held, pos, scale[0], scale[1], *tables))
    scale = (scale0, scale1)
    others = send(held, SWAP)

    up_plane = second_line(first_line(jnp.concatenate(up_own, axis=0), FIRST), SECOND)
    down_plane = second_line(first_line(jnp.concatenate(down_own, axis=0), FIRST), SECOND)

    act = [up_call(part, pos, held, others, scale[part], up_plane) for part in range(2)]
    act += [send(h, SWAP) for h in act]

    mine, theirs = [], []
    for batch, refs in enumerate((down_plane[:4], down_plane[4:])):
        own, low, high = down_call(batch, pos, act, refs)
        above, below = send(low, DOWNWARD), send(high, UPWARD)
        kept, sent = sum_call(pos, own, above, below, tables[batch])
        mine.append(kept)
        theirs.append(send(sent, SWAP))
    return last_call(pos, *mine, *theirs)


def solution(mesh):
    fine = Mesh(mesh.devices.reshape(2, 2, 4, 4, 2), AXES)
    fs = ("zl", "y", "x")
    rows = P(AXES, None)
    placed = (rows, P(), P(fs, "c"), P("c"), P("c", fs), P())
    return jax.shard_map(body, mesh=fine, in_specs=placed, out_specs=rows, check_vma=False)
```

```python
import functools

import jax
import jax.numpy as jnp
from jax import lax
from jax.experimental import pallas as pl
from jax.experimental.pallas import tpu as pltpu
from jax.sharding import Mesh, PartitionSpec as P


AXES = ("zh", "zl", "y", "x", "c")
NEAR = (0, -1, 1, 2)
BLOCK = 64
LINE = 4 * BLOCK
CHUNK = 256
COLUMNS = (2 * LINE, 2 * LINE)
ANY = pl.BlockSpec(memory_space=pl.ANY)
SMEM = pl.BlockSpec(memory_space=pltpu.SMEM)
VMEM = pl.BlockSpec(memory_space=pltpu.VMEM)
BF16 = jnp.bfloat16


def index_of(z, y, x, c):
    return ((z % 4 * 4 + y % 4) * 4 + x % 4) * 2 + c


def pairs_of(target):
    pairs = []
    for z in range(4):
        for y in range(4):
            for x in range(4):
                for c in range(2):
                    to = target(z, y, x, c)
                    if to is not None:
                        pairs.append((index_of(z, y, x, c), index_of(*to)))
    return pairs


def first_ring(d):
    return pairs_of(lambda z, y, x, c: (z, y + d, x, c) if c else (z, y, x + d, c))


def second_ring(d):
    return pairs_of(lambda z, y, x, c: (z, y, x + d, c) if c else (z, y + d, x, c))


def z_ring(d):
    return pairs_of(lambda z, y, x, c: (z + d, y, x, c))


FIRST = (first_ring(1), first_ring(-1))
SECOND = (second_ring(1), second_ring(-1))
UPWARD, DOWNWARD = z_ring(1), z_ring(-1)
SWAP = pairs_of(lambda z, y, x, c: (z, y, x, 1 - c))


def to_lower(z, y, x, c):
    if c == 0:
        return z - 1, y, x, z % 2
    return (z, y, x, 0) if z % 2 == 0 else None


def to_upper(z, y, x, c):
    if c == 1:
        return z + 1, y, x, z % 2
    return (z, y, x, 1) if z % 2 == 1 else None


TO_LOWER, TO_UPPER = pairs_of(to_lower), pairs_of(to_upper)


def send(a, pairs):
    return lax.ppermute(a, AXES, pairs)


def first_line(own, ring):
    before, after = send(own, ring[0]), send(own, ring[1])
    n = own.shape[0] // 2
    far = send(before[:n], ring[0]), send(after[n:], ring[1])
    return jnp.concatenate([own, before], axis=0), jnp.concatenate([after, *far], axis=0)


def second_line(own, ring):
    low, high = own
    low_before, low_after = send(low, ring[0]), send(low, ring[1])
    high_before, high_after = send(high, ring[0]), send(high, ring[1])
    far = send(low_before, ring[0]), send(high_after, ring[1])
    return low, high, low_before, high_before, low_after, high_after, *far


def near(value, shift):
    return lax.rem(value + (shift + 4), 4)


def parts_of(refs):
    return [(ref, i, NEAR[k // 2], NEAR[k % 2 * 2 + i]) for k, ref in enumerate(refs) for i in range(2)]


def up_kernel(first, pos, x0, x1, scale, *refs):
    refs, (act, wv, wsem) = refs[:8], refs[8:]
    a, b, sa, sb, core = pos[0], pos[1], pos[2], pos[3], pos[4]
    width, n = wv.shape
    held = x0.shape[0]
    chunks = n // CHUNK

    def w_start(j):
        for ref, i, d, e in parts_of(refs):
            for level in range(2):
                at = pl.multiple_of(level * (width // 2) + near(a, e) * sa + near(b, d) * sb, BLOCK)
                pltpu.make_async_copy(
                    ref.at[pl.ds((2 * i + level) * BLOCK, BLOCK), pl.ds(first + j * CHUNK, CHUNK)],
                    wv.at[pl.ds(at, BLOCK), pl.ds(j * CHUNK, CHUNK)],
                    wsem.at[j],
                ).start()

    def w_wait(j):
        cols = pl.ds(pl.multiple_of(j * CHUNK, CHUNK), CHUNK)
        pltpu.make_async_copy(wv.at[:, cols], wv.at[:, cols], wsem.at[j]).wait()

    w_start(0)
    w_wait(0)
    for j in range(1, chunks):
        w_start(j)

    def chunk(j, carry):
        cols = pl.ds(pl.multiple_of(j * CHUNK, CHUNK), CHUNK)

        @pl.when(j > 0)
        def _():
            w_wait(j)

        for ref, who in ((x0, core), (x1, 1 - core)):
            pre = jnp.dot(ref[...], wv[:, cols], preferred_element_type=jnp.float32)
            pre = jnp.maximum(pre * scale[:, cols], 0.0)
            act[pl.ds(pl.multiple_of(who * held, held), held), cols] = (pre * pre).astype(BF16)
        return carry

    lax.fori_loop(0, chunks, chunk, 0)


def up_call(part, pos, x0, x1, scale, weights):
    rows, width = 2 * x0.shape[0], x0.shape[1]
    n = scale.shape[1]
    return pl.pallas_call(
        functools.partial(up_kernel, part * n),
        out_shape=jax.ShapeDtypeStruct((rows, n), BF16),
        in_specs=[SMEM, VMEM, VMEM, VMEM] + [ANY] * 8,
        out_specs=VMEM,
        scratch_shapes=[
            pltpu.VMEM((width, n), BF16),
            pltpu.SemaphoreType.DMA((n // CHUNK,)),
        ],
        compiler_params=pltpu.CompilerParams(vmem_limit_bytes=14 * 2**20),
        cost_estimate=pl.CostEstimate(flops=2 * rows * width * n, bytes_accessed=2 * (rows * width + width * n + rows * n), transcendentals=0),
    )(pos, x0, x1, scale, *weights)


def down_kernel(pos, h0, h1, o0, o1, *refs):
    refs, (own, low, high, vv, ov, vsem, osem) = refs[:-7], refs[-7:]
    a = pos[0]
    rows, quarter = h0.shape
    kept = rows // 4
    half = kept // 2

    def v_start(g):
        for k, ref in enumerate(refs[2 * g : 2 * g + 2]):
            for i in range(4):
                at = pl.multiple_of(g * LINE + near(a, NEAR[2 * k + i // 2]) * BLOCK, BLOCK)
                pltpu.make_async_copy(
                    ref.at[pl.ds(i * BLOCK, BLOCK)],
                    vv.at[pl.ds(at, BLOCK), pl.ds(i % 2 * 2 * quarter, 2 * quarter)],
                    vsem.at[g],
                ).start()

    groups = vv.shape[0] // LINE
    for g in range(groups):
        v_start(g)

    def out_copies(c):
        rows_of = ((own, 0, kept), (low, kept, half), (high, kept + half, half))
        return [
            pltpu.make_async_copy(
                ov.at[pl.ds(c * 2 * kept + start, size)], ref.at[pl.ds(c * size, size)], osem.at[3 * c + i]
            )
            for i, (ref, start, size) in enumerate(rows_of)
        ]

    def chunk(k, carry):
        r = pl.ds(pl.multiple_of(k * 2 * kept, 2 * kept), 2 * kept)

        def one(g, carry):
            cols = pl.ds(pl.multiple_of(g * LINE, LINE), LINE)

            @pl.when(k == 0)
            def _():
                pltpu.make_async_copy(vv.at[cols], vv.at[cols], vsem.at[g]).wait()

            part = None
            for q, ref in enumerate((h0, h1, o0, o1)):
                term = lax.dot_general(
                    ref[r, :],
                    vv[cols, pl.ds(q * quarter, quarter)],
                    (((1,), (1,)), ((), ())),
                    preferred_element_type=jnp.float32,
                )
                part = term if part is None else part + term
            ov[r, cols] = part.astype(BF16)
            return carry

        lax.fori_loop(0, groups, one, 0)
        for c in range(2):

            @pl.when(k == c)
            def _():
                for copy in out_copies(c):
                    copy.start()

        return carry

    lax.fori_loop(0, 2, chunk, 0)
    for c in range(2):
        for copy in out_copies(c):
            copy.wait()


def down_call(batch, pos, act, refs):
    rows, units = act[0].shape[0], 4 * act[0].shape[1]
    n = COLUMNS[batch]
    return pl.pallas_call(
        down_kernel,
        out_shape=[jax.ShapeDtypeStruct((rows // k, n), BF16) for k in (2, 4, 4)],
        in_specs=[SMEM] + [VMEM] * 4 + [ANY] * len(refs),
        out_specs=[ANY] * 3,
        scratch_shapes=[
            pltpu.VMEM((n, units), BF16),
            pltpu.VMEM((rows, n), BF16),
            pltpu.SemaphoreType.DMA((n // LINE,)),
            pltpu.SemaphoreType.DMA((6,)),
        ],
        compiler_params=pltpu.CompilerParams(vmem_limit_bytes=14 * 2**20),
        cost_estimate=pl.CostEstimate(flops=2 * rows * units * n, bytes_accessed=2 * (rows * units + units * n + rows * n), transcendentals=0),
    )(pos, *act, *refs)


def sum_kernel(pos, own, above, below, gain, mine, theirs):
    core = pos[4]
    kept = mine.shape[0]
    half = kept // 2
    for ref, who in ((mine, core), (theirs, 1 - core)):
        for i, other in enumerate((above, below)):
            r = pl.ds(pl.multiple_of(who * kept + i * half, half), half)
            total = own[r, :].astype(jnp.float32) + other[pl.ds(pl.multiple_of(who * half, half), half), :].astype(jnp.float32)
            ref[pl.ds(i * half, half), :] = (total * gain[...]).astype(BF16)


def sum_call(pos, own, above, below, gain):
    shape = jax.ShapeDtypeStruct((own.shape[0] // 2, own.shape[1]), BF16)
    return pl.pallas_call(
        sum_kernel,
        out_shape=[shape, shape],
        in_specs=[SMEM, VMEM, VMEM, VMEM, VMEM],
        out_specs=[VMEM, VMEM],
        compiler_params=pltpu.CompilerParams(vmem_limit_bytes=6 * 2**20),
    )(pos, own, above, below, gain)


def last_kernel(pos, m0, m1, g0, g1, out, qv, ov, dsem, qsem, osem):
    core, y, x = pos[4], pos[5], pos[6]
    half = ov.shape[1]

    def pieces(near_two, far_two):
        refs = ((near_two, 0), (near_two, 1), (far_two, 0), (far_two, 1))
        return [(ref.at[:, pl.ds(i * LINE, LINE)], d) for (ref, i), d in zip(refs, NEAR)]

    def start(straight, mixed):
        for ref, d in straight:
            at = pl.multiple_of(near(y, d) * LINE, LINE)
            pltpu.make_async_copy(ref, out.at[:, pl.ds(at, LINE)], dsem.at[0]).start()
        for ref, d in mixed:
            pltpu.make_async_copy(ref, qv.at[near(x, d)], qsem.at[0]).start()

    @pl.when(core == 0)
    def _():
        start(pieces(m0, m1), pieces(g0, g1))

    @pl.when(core == 1)
    def _():
        start(pieces(g0, g1), pieces(m0, m1))

    pltpu.make_async_copy(qv, qv, qsem.at[0]).wait()
    left = lax.broadcasted_iota(jnp.int32, (qv.shape[1], 128), 1) < BLOCK
    for pair in range(2):
        for v in range(2):
            cols = pl.ds(128 * v, 128)
            even = qv[2 * pair, :, cols].astype(jnp.float32)
            odd = qv[2 * pair + 1, :, cols].astype(jnp.float32)
            ov[:, pl.ds(2 * v * LINE + pair * 128, 128)] = jnp.where(left, even, pltpu.roll(odd, BLOCK, 1)).astype(BF16)
            ov[:, pl.ds((2 * v + 1) * LINE + pair * 128, 128)] = jnp.where(left, pltpu.roll(even, BLOCK, 1), odd).astype(BF16)
    copy = pltpu.make_async_copy(ov, out.at[:, pl.ds(half, half)], osem.at[0])
    copy.start()
    copy.wait()
    pltpu.make_async_copy(ov, out.at[:, pl.ds(0, half)], dsem.at[0]).wait()


def last_call(pos, *refs):
    rows = refs[0].shape[0]
    return pl.pallas_call(
        last_kernel,
        name="last",
        out_shape=jax.ShapeDtypeStruct((rows, 8 * LINE), BF16),
        in_specs=[SMEM] + [ANY] * 4,
        out_specs=ANY,
        scratch_shapes=[
            pltpu.VMEM((4, rows, LINE), BF16),
            pltpu.VMEM((rows, 4 * LINE), BF16),
            pltpu.SemaphoreType.DMA((1,)),
            pltpu.SemaphoreType.DMA((1,)),
            pltpu.SemaphoreType.DMA((1,)),
        ],
        compiler_params=pltpu.CompilerParams(vmem_limit_bytes=6 * 2**20),
    )(pos, *refs)


def body(hidden_in, norm_gain, up_weight, up_scale, down_weight, down_scale):
    zl, y, x, core = (lax.axis_index(name) for name in ("zl", "y", "x", "c"))
    a, b = jnp.where(core == 0, x, y), jnp.where(core == 0, y, x)
    sa, sb = jnp.where(core == 0, BLOCK, LINE), jnp.where(core == 0, LINE, BLOCK)
    pos = jnp.stack([a, b, sa, sb, core, y, x]).astype(jnp.int32)
    tokens, _ = hidden_in.shape
    units = up_weight.shape[1] // 2
    half = tokens // 2

    def halves_of(shard):
        mine = lax.dynamic_slice_in_dim(shard, zl * units, units, 1)
        return mine, lax.dynamic_slice_in_dim(shard, (1 - zl) * units, units, 1)

    mine, theirs = halves_of(up_weight.astype(BF16))
    other = send(theirs, DOWNWARD)
    up_own = [jnp.where(zl == 0, mine, other), jnp.where(zl == 0, other, mine)]

    hidden_in, up_own[0] = lax.optimization_barrier((hidden_in, up_own[0]))

    mine, theirs = halves_of(down_weight.astype(BF16).T)
    lower = send(jnp.where(core == 0, theirs, mine), TO_LOWER)
    upper = send(jnp.where(core == 1, theirs, mine), TO_UPPER)
    ra, rb = jnp.where(core == 0, lower, upper), jnp.where(core == 0, upper, lower)
    down_own = [jnp.where(core == zl, mine, ra), jnp.where(core == zl, ra, rb)]

    f32 = hidden_in.astype(jnp.float32)
    normed = (
        f32 * lax.rsqrt(jnp.mean(f32 * f32, axis=1, keepdims=True) + 1e-06) * norm_gain
    ).astype(BF16)
    held = jnp.concatenate([normed, send(normed[:half], UPWARD), send(normed[half:], DOWNWARD)], axis=0)
    scale = lax.dynamic_slice_in_dim(up_scale, zl * units, units, 0).reshape(2, 1, units // 2)
    gain = lax.dynamic_index_in_dim(down_scale.reshape(2, 4, 4, BLOCK), core, 0, keepdims=False)
    gain = jnp.where(core == 0, gain, jnp.swapaxes(gain, 0, 1)).reshape(4, LINE)
    gain = jnp.concatenate([lax.dynamic_slice_in_dim(gain, near(b, d), 1, 0) for d in NEAR], axis=1)
    tables = [gain[:, : COLUMNS[0]], gain[:, COLUMNS[0] :]]
    held, pos, scale0, scale1, *tables = lax.optimization_barrier((held, pos, scale[0], scale[1], *tables))
    scale = (scale0, scale1)
    others = send(held, SWAP)

    up_plane = second_line(first_line(jnp.concatenate(up_own, axis=0), FIRST), SECOND)
    down_plane = second_line(first_line(jnp.concatenate(down_own, axis=0), FIRST), SECOND)

    act = [up_call(part, pos, held, others, scale[part], up_plane) for part in range(2)]
    act += [send(h, SWAP) for h in act]

    mine, theirs = [], []
    for batch, refs in enumerate((down_plane[:4], down_plane[4:])):
        own, low, high = down_call(batch, pos, act, refs)
        above, below = send(low, DOWNWARD), send(high, UPWARD)
        kept, sent = sum_call(pos, own, above, below, tables[batch])
        mine.append(kept)
        theirs.append(send(sent, SWAP))
    return last_call(pos, *mine, *theirs)


def solution(mesh):
    fine = Mesh(mesh.devices.reshape(2, 2, 4, 4, 2), AXES)
    fs = ("zl", "y", "x")
    rows = P(AXES, None)
    placed = (rows, P(), P(fs, "c"), P("c"), P("c", fs), P())
    return jax.shard_map(body, mesh=fine, in_specs=placed, out_specs=rows, check_vma=False)
```

```python
import functools

import jax
import jax.numpy as jnp
from jax import lax
from jax.experimental import pallas as pl
from jax.experimental.pallas import tpu as pltpu
from jax.sharding import Mesh, PartitionSpec as P


AXES = ("zh", "zl", "y", "x", "c")
NEAR = (0, -1, 1, 2)
BLOCK = 64
LINE = 4 * BLOCK
CHUNK = 256
COLUMNS = (2 * LINE, 2 * LINE)
UNITS = (1280, 768)
ANY = pl.BlockSpec(memory_space=pl.ANY)
SMEM = pl.BlockSpec(memory_space=pltpu.SMEM)
VMEM = pl.BlockSpec(memory_space=pltpu.VMEM)
BF16 = jnp.bfloat16


def index_of(z, y, x, c):
    return ((z % 4 * 4 + y % 4) * 4 + x % 4) * 2 + c


def pairs_of(target):
    pairs = []
    for z in range(4):
        for y in range(4):
            for x in range(4):
                for c in range(2):
                    to = target(z, y, x, c)
                    if to is not None:
                        pairs.append((index_of(z, y, x, c), index_of(*to)))
    return pairs


def first_ring(d):
    return pairs_of(lambda z, y, x, c: (z, y + d, x, c) if c else (z, y, x + d, c))


def second_ring(d):
    return pairs_of(lambda z, y, x, c: (z, y, x + d, c) if c else (z, y + d, x, c))


def z_ring(d):
    return pairs_of(lambda z, y, x, c: (z + d, y, x, c))


FIRST = (first_ring(1), first_ring(-1))
SECOND = (second_ring(1), second_ring(-1))
UPWARD, DOWNWARD = z_ring(1), z_ring(-1)
SWAP = pairs_of(lambda z, y, x, c: (z, y, x, 1 - c))


def to_lower(z, y, x, c):
    if c == 0:
        return z - 1, y, x, z % 2
    return (z, y, x, 0) if z % 2 == 0 else None


def to_upper(z, y, x, c):
    if c == 1:
        return z + 1, y, x, z % 2
    return (z, y, x, 1) if z % 2 == 1 else None


TO_LOWER, TO_UPPER = pairs_of(to_lower), pairs_of(to_upper)


def send(a, pairs):
    return lax.ppermute(a, AXES, pairs)


def first_line(own, ring):
    before, after = send(own, ring[0]), send(own, ring[1])
    n = own.shape[0] // 2
    far = send(before[:n], ring[0]), send(after[n:], ring[1])
    return jnp.concatenate([own, before], axis=0), jnp.concatenate([after, *far], axis=0)


def second_line(own, ring):
    low, high = own
    low_before, low_after = send(low, ring[0]), send(low, ring[1])
    high_before, high_after = send(high, ring[0]), send(high, ring[1])
    far = send(low_before, ring[0]), send(high_after, ring[1])
    return low, high, low_before, high_before, low_after, high_after, *far


def near(value, shift):
    return lax.rem(value + (shift + 4), 4)


def parts_of(refs):
    return [(ref, i, NEAR[k // 2], NEAR[k % 2 * 2 + i]) for k, ref in enumerate(refs) for i in range(2)]


def up_kernel(first, pos, x0, x1, scale, *refs):
    refs, (act, wv, wsem) = refs[:8], refs[8:]
    a, b, sa, sb, core = pos[0], pos[1], pos[2], pos[3], pos[4]
    width, n = wv.shape
    held = x0.shape[0]
    chunks = n // CHUNK

    def w_start(j):
        for ref, i, d, e in parts_of(refs):
            for level in range(2):
                at = pl.multiple_of(level * (width // 2) + near(a, e) * sa + near(b, d) * sb, BLOCK)
                pltpu.make_async_copy(
                    ref.at[pl.ds((2 * i + level) * BLOCK, BLOCK), pl.ds(first + j * CHUNK, CHUNK)],
                    wv.at[pl.ds(at, BLOCK), pl.ds(j * CHUNK, CHUNK)],
                    wsem.at[j],
                ).start()

    def w_wait(j):
        cols = pl.ds(pl.multiple_of(j * CHUNK, CHUNK), CHUNK)
        pltpu.make_async_copy(wv.at[:, cols], wv.at[:, cols], wsem.at[j]).wait()

    w_start(0)
    w_wait(0)
    for j in range(1, chunks):
        w_start(j)

    def chunk(j, carry):
        cols = pl.ds(pl.multiple_of(j * CHUNK, CHUNK), CHUNK)

        @pl.when(j > 0)
        def _():
            w_wait(j)

        for ref, who in ((x0, core), (x1, 1 - core)):
            pre = jnp.dot(ref[...], wv[:, cols], preferred_element_type=jnp.float32)
            pre = jnp.maximum(pre * scale[:, cols], 0.0)
            act[pl.ds(pl.multiple_of(who * held, held), held), cols] = (pre * pre).astype(BF16)
        return carry

    lax.fori_loop(0, chunks, chunk, 0)


def up_call(part, pos, x0, x1, scale, weights):
    rows, width = 2 * x0.shape[0], x0.shape[1]
    n = scale.shape[1]
    return pl.pallas_call(
        functools.partial(up_kernel, part * UNITS[0]),
        out_shape=jax.ShapeDtypeStruct((rows, n), BF16),
        in_specs=[SMEM, VMEM, VMEM, VMEM] + [ANY] * 8,
        out_specs=VMEM,
        scratch_shapes=[
            pltpu.VMEM((width, n), BF16),
            pltpu.SemaphoreType.DMA((n // CHUNK,)),
        ],
        compiler_params=pltpu.CompilerParams(vmem_limit_bytes=14 * 2**20),
        cost_estimate=pl.CostEstimate(flops=2 * rows * width * n, bytes_accessed=2 * (rows * width + width * n + rows * n), transcendentals=0),
    )(pos, x0, x1, scale, *weights)


def down_kernel(pos, h0, h1, o0, o1, *refs):
    refs, (own, low, high, vv, ov, vsem, osem) = refs[:-7], refs[-7:]
    a = pos[0]
    rows, units = h0.shape[0], sum(UNITS)
    kept = rows // 4
    half = kept // 2

    def v_start(g):
        for k, ref in enumerate(refs[2 * g : 2 * g + 2]):
            for i in range(4):
                at = pl.multiple_of(g * LINE + near(a, NEAR[2 * k + i // 2]) * BLOCK, BLOCK)
                pltpu.make_async_copy(
                    ref.at[pl.ds(i * BLOCK, BLOCK)],
                    vv.at[pl.ds(at, BLOCK), pl.ds(i % 2 * units, units)],
                    vsem.at[g],
                ).start()

    groups = vv.shape[0] // LINE
    for g in range(groups):
        v_start(g)

    def out_copies(c):
        rows_of = ((own, 0, kept), (low, kept, half), (high, kept + half, half))
        return [
            pltpu.make_async_copy(
                ov.at[pl.ds(c * 2 * kept + start, size)], ref.at[pl.ds(c * size, size)], osem.at[3 * c + i]
            )
            for i, (ref, start, size) in enumerate(rows_of)
        ]

    def chunk(k, carry):
        r = pl.ds(pl.multiple_of(k * 2 * kept, 2 * kept), 2 * kept)

        def one(g, carry):
            cols = pl.ds(pl.multiple_of(g * LINE, LINE), LINE)

            @pl.when(k == 0)
            def _():
                pltpu.make_async_copy(vv.at[cols], vv.at[cols], vsem.at[g]).wait()

            part = None
            for first, ref in ((0, h0), (UNITS[0], h1), (units, o0), (units + UNITS[0], o1)):
                term = lax.dot_general(
                    ref[r, :],
                    vv[cols, pl.ds(first, ref.shape[1])],
                    (((1,), (1,)), ((), ())),
                    preferred_element_type=jnp.float32,
                )
                part = term if part is None else part + term
            ov[r, cols] = part.astype(BF16)
            return carry

        lax.fori_loop(0, groups, one, 0)
        for c in range(2):

            @pl.when(k == c)
            def _():
                for copy in out_copies(c):
                    copy.start()

        return carry

    lax.fori_loop(0, 2, chunk, 0)
    for c in range(2):
        for copy in out_copies(c):
            copy.wait()


def down_call(batch, pos, act, refs):
    rows, units = act[0].shape[0], 2 * sum(UNITS)
    n = COLUMNS[batch]
    return pl.pallas_call(
        down_kernel,
        out_shape=[jax.ShapeDtypeStruct((rows // k, n), BF16) for k in (2, 4, 4)],
        in_specs=[SMEM] + [VMEM] * 4 + [ANY] * len(refs),
        out_specs=[ANY] * 3,
        scratch_shapes=[
            pltpu.VMEM((n, units), BF16),
            pltpu.VMEM((rows, n), BF16),
            pltpu.SemaphoreType.DMA((n // LINE,)),
            pltpu.SemaphoreType.DMA((6,)),
        ],
        compiler_params=pltpu.CompilerParams(vmem_limit_bytes=14 * 2**20),
        cost_estimate=pl.CostEstimate(flops=2 * rows * units * n, bytes_accessed=2 * (rows * units + units * n + rows * n), transcendentals=0),
    )(pos, *act, *refs)


def sum_kernel(pos, own, above, below, gain, mine, theirs):
    core = pos[4]
    kept = mine.shape[0]
    half = kept // 2
    for ref, who in ((mine, core), (theirs, 1 - core)):
        for i, other in enumerate((above, below)):
            r = pl.ds(pl.multiple_of(who * kept + i * half, half), half)
            total = own[r, :].astype(jnp.float32) + other[pl.ds(pl.multiple_of(who * half, half), half), :].astype(jnp.float32)
            ref[pl.ds(i * half, half), :] = (total * gain[...]).astype(BF16)


def sum_call(pos, own, above, below, gain):
    shape = jax.ShapeDtypeStruct((own.shape[0] // 2, own.shape[1]), BF16)
    return pl.pallas_call(
        sum_kernel,
        out_shape=[shape, shape],
        in_specs=[SMEM, VMEM, VMEM, VMEM, VMEM],
        out_specs=[VMEM, VMEM],
        compiler_params=pltpu.CompilerParams(vmem_limit_bytes=6 * 2**20),
    )(pos, own, above, below, gain)


def last_kernel(pos, m0, m1, g0, g1, out, qv, ov, dsem, qsem, osem):
    core, y, x = pos[4], pos[5], pos[6]
    half = ov.shape[1]

    def pieces(near_two, far_two):
        refs = ((near_two, 0), (near_two, 1), (far_two, 0), (far_two, 1))
        return [(ref.at[:, pl.ds(i * LINE, LINE)], d) for (ref, i), d in zip(refs, NEAR)]

    def start(straight, mixed):
        for ref, d in straight:
            at = pl.multiple_of(near(y, d) * LINE, LINE)
            pltpu.make_async_copy(ref, out.at[:, pl.ds(at, LINE)], dsem.at[0]).start()
        for ref, d in mixed:
            pltpu.make_async_copy(ref, qv.at[near(x, d)], qsem.at[0]).start()

    @pl.when(core == 0)
    def _():
        start(pieces(m0, m1), pieces(g0, g1))

    @pl.when(core == 1)
    def _():
        start(pieces(g0, g1), pieces(m0, m1))

    pltpu.make_async_copy(qv, qv, qsem.at[0]).wait()
    left = lax.broadcasted_iota(jnp.int32, (qv.shape[1], 128), 1) < BLOCK
    for pair in range(2):
        for v in range(2):
            cols = pl.ds(128 * v, 128)
            even = qv[2 * pair, :, cols].astype(jnp.float32)
            odd = qv[2 * pair + 1, :, cols].astype(jnp.float32)
            ov[:, pl.ds(2 * v * LINE + pair * 128, 128)] = jnp.where(left, even, pltpu.roll(odd, BLOCK, 1)).astype(BF16)
            ov[:, pl.ds((2 * v + 1) * LINE + pair * 128, 128)] = jnp.where(left, pltpu.roll(even, BLOCK, 1), odd).astype(BF16)
    copy = pltpu.make_async_copy(ov, out.at[:, pl.ds(half, half)], osem.at[0])
    copy.start()
    copy.wait()
    pltpu.make_async_copy(ov, out.at[:, pl.ds(0, half)], dsem.at[0]).wait()


def last_call(pos, *refs):
    rows = refs[0].shape[0]
    return pl.pallas_call(
        last_kernel,
        name="last",
        out_shape=jax.ShapeDtypeStruct((rows, 8 * LINE), BF16),
        in_specs=[SMEM] + [ANY] * 4,
        out_specs=ANY,
        scratch_shapes=[
            pltpu.VMEM((4, rows, LINE), BF16),
            pltpu.VMEM((rows, 4 * LINE), BF16),
            pltpu.SemaphoreType.DMA((1,)),
            pltpu.SemaphoreType.DMA((1,)),
            pltpu.SemaphoreType.DMA((1,)),
        ],
        compiler_params=pltpu.CompilerParams(vmem_limit_bytes=6 * 2**20),
    )(pos, *refs)


def body(hidden_in, norm_gain, up_weight, up_scale, down_weight, down_scale):
    zl, y, x, core = (lax.axis_index(name) for name in ("zl", "y", "x", "c"))
    a, b = jnp.where(core == 0, x, y), jnp.where(core == 0, y, x)
    sa, sb = jnp.where(core == 0, BLOCK, LINE), jnp.where(core == 0, LINE, BLOCK)
    pos = jnp.stack([a, b, sa, sb, core, y, x]).astype(jnp.int32)
    tokens, _ = hidden_in.shape
    units = up_weight.shape[1] // 2
    half = tokens // 2

    def halves_of(shard):
        mine = lax.dynamic_slice_in_dim(shard, zl * units, units, 1)
        return mine, lax.dynamic_slice_in_dim(shard, (1 - zl) * units, units, 1)

    mine, theirs = halves_of(up_weight.astype(BF16))
    other = send(theirs, DOWNWARD)
    up_own = [jnp.where(zl == 0, mine, other), jnp.where(zl == 0, other, mine)]

    hidden_in, up_own[0] = lax.optimization_barrier((hidden_in, up_own[0]))

    mine, theirs = halves_of(down_weight.astype(BF16).T)
    lower = send(jnp.where(core == 0, theirs, mine), TO_LOWER)
    upper = send(jnp.where(core == 1, theirs, mine), TO_UPPER)
    ra, rb = jnp.where(core == 0, lower, upper), jnp.where(core == 0, upper, lower)
    down_own = [jnp.where(core == zl, mine, ra), jnp.where(core == zl, ra, rb)]

    f32 = hidden_in.astype(jnp.float32)
    normed = (
        f32 * lax.rsqrt(jnp.mean(f32 * f32, axis=1, keepdims=True) + 1e-06) * norm_gain
    ).astype(BF16)
    held = jnp.concatenate([normed, send(normed[:half], UPWARD), send(normed[half:], DOWNWARD)], axis=0)
    scale = lax.dynamic_slice_in_dim(up_scale, zl * units, units, 0).reshape(1, units)
    gain = lax.dynamic_index_in_dim(down_scale.reshape(2, 4, 4, BLOCK), core, 0, keepdims=False)
    gain = jnp.where(core == 0, gain, jnp.swapaxes(gain, 0, 1)).reshape(4, LINE)
    gain = jnp.concatenate([lax.dynamic_slice_in_dim(gain, near(b, d), 1, 0) for d in NEAR], axis=1)
    tables = [gain[:, : COLUMNS[0]], gain[:, COLUMNS[0] :]]
    held, pos, scale0, scale1, *tables = lax.optimization_barrier((held, pos, scale[:, : UNITS[0]], scale[:, UNITS[0] :], *tables))
    scale = (scale0, scale1)
    others = send(held, SWAP)

    up_plane = second_line(first_line(jnp.concatenate(up_own, axis=0), FIRST), SECOND)
    down_plane = second_line(first_line(jnp.concatenate(down_own, axis=0), FIRST), SECOND)

    act = [up_call(part, pos, held, others, scale[part], up_plane) for part in range(2)]
    act += [send(h, SWAP) for h in act]

    mine, theirs = [], []
    for batch, refs in enumerate((down_plane[:4], down_plane[4:])):
        own, low, high = down_call(batch, pos, act, refs)
        above, below = send(low, DOWNWARD), send(high, UPWARD)
        kept, sent = sum_call(pos, own, above, below, tables[batch])
        mine.append(kept)
        theirs.append(send(sent, SWAP))
    return last_call(pos, *mine, *theirs)


def solution(mesh):
    fine = Mesh(mesh.devices.reshape(2, 2, 4, 4, 2), AXES)
    fs = ("zl", "y", "x")
    rows = P(AXES, None)
    placed = (rows, P(), P(fs, "c"), P("c"), P("c", fs), P())
    return jax.shard_map(body, mesh=fine, in_specs=placed, out_specs=rows, check_vma=False)
```
